256 devices in a mesh: ep: 64 (over z, y, core), tp: 4 (over x).
Axes of the slice: x: 4, y: 4, z: 8, core: 2. Of those that a mesh axis runs over, the one named last changes fastest.
Arguments:
- tokens: bfloat16 [1024, 2048], P('ep'), may hold values from -6 to 6
- recur_state: float32 [1024, 8, 128, 128], P('ep', 'tp'), may hold values from -0.4 to 0.4
- attn_gain: float32 [2048], replicated, may hold values from 0.1 to 1.9
- query_weight: bfloat16 [2048, 1024], P(None, 'tp'), may hold values from -0.125 to 0.125
- key_weight: bfloat16 [2048, 1024], P(None, 'tp'), may hold values from -0.125 to 0.125
- value_weight: bfloat16 [2048, 1024], P(None, 'tp'), may hold values from -0.125 to 0.125
- outgate_weight: bfloat16 [2048, 1024], P(None, 'tp'), may hold values from -0.125 to 0.125
- beta_weight: bfloat16 [2048, 8], replicated, may hold values from -0.125 to 0.125
- decay_weight: bfloat16 [2048, 8], replicated, may hold values from -0.125 to 0.125
- decay_rate: float32 [8], replicated, may hold values from 0.05 to 2
- head_gain: float32 [128], replicated, may hold values from 0.1 to 1.9
- output_weight: bfloat16 [1024, 2048], P('tp'), may hold values from -0.1875 to 0.1875
- ffn_gain: float32 [2048], replicated, may hold values from 0.1 to 1.9
- routes: int32 [1024, 2], P('ep'), may hold values from 0 to 15, all different within a row; in each aligned block of 16 rows (0 to 15, 16 to 31, ...) at most 4 rows name the same one
- route_weight: float32 [1024, 2], P('ep'), may hold values from 0.2 to 1
- expert_gate: bfloat16 [64, 2048, 1024], P('ep', None, 'tp'), may hold values from -0.125 to 0.125
- expert_up: bfloat16 [64, 2048, 1024], P('ep', None, 'tp'), may hold values from -0.125 to 0.125
- expert_down: bfloat16 [64, 1024, 2048], P('ep', 'tp'), may hold values from -0.09375 to 0.09375
Outputs:
- mixed: bfloat16 [1024, 2048], P('ep', 'tp')
- new_state: float32 [1024, 8, 128, 128], P('ep', 'tp')
The draws below stay inside these ranges and needn't reach their ends.
Inputs may be any that keep to these rules, and one draw needn't show every extreme that they name: `routes`: each row names 2 different experts; in each aligned block of 16 rows no expert is named by more than 4 rows.
All inputs are finite; a program needn't handle non-finite values.
Results may differ from the reference program's by a relative error of at most 0.014.
Values may be sent and summed in bfloat16 or wider, within the bound.
A program may use at most 64 MiB of HBM per device.

```python
import math
import jax
import jax.numpy as jnp
import numpy as np
from jax import lax

D = 2048
H = 8
HEAD = 128
FF_E = 4096
TOP = 2
SEQ_DEV = 16
TOKENS = 1024
EXPERTS = 16
FF_PART = 1024
CAP = 4
N_EP = 64


def levels(key, shape, cuts, low, largest):
    def one(dim, shards_of):
        steps = jax.random.uniform(jax.random.fold_in(jax.random.fold_in(key, 6), dim), (shards_of,), jnp.float32, low / len(cuts), largest / len(cuts))
        return jnp.repeat(jnp.exp(steps), shape[dim] // shards_of).reshape((-1,) + (1,) * (len(shape) - dim - 1))

    level = one(*cuts[0])
    for cut in cuts[1:]:
        level = level * one(*cut)
    return level


def shared_out(rng, own, number, rows, count, top, reach, lean):
    order = jax.random.permutation(rng, count)
    crowded, ordinary = load_shares(count, rows * top, reach, lean, True), load_shares(count, rows * top, reach, lean, False)
    places = jnp.arange(count)

    def named(sizes, offset_by):
        used = int((sizes > 0).sum())
        fixed = max(1, used // 4)
        passed = fixed + (places - fixed + offset_by * (used - fixed)) % max(1, count - fixed)
        return jnp.zeros((count,), jnp.int32).at[order[jnp.where(places < fixed, places, passed)]].set(jnp.asarray(sizes, jnp.int32))

    sizes = jnp.where(number % 4 == 0, named(crowded, number // 4), named(ordinary, number - number // 4 - 1))
    mixed = jax.random.permutation(jax.random.fold_in(own, 3), count)
    donor, sink = mixed[0:count // 2 * 2:2], mixed[1:count // 2 * 2:2]
    room = jnp.minimum(sizes[donor] - 1, reach - sizes[sink]) // 2
    room = jnp.where((donor == order[0]) | (sink == order[0]) | (sizes[sink] == 0), 0, jnp.maximum(room, 0))
    passed = jax.random.randint(jax.random.fold_in(own, 4), (count // 2,), 0, 1 << 20) % (room + 1)
    sizes = sizes.at[donor].add(-passed).at[sink].add(passed)
    members = jnp.searchsorted(jnp.cumsum(sizes), jnp.arange(rows * top), side="right").astype(jnp.int32)
    listing = members.reshape(top, rows).T
    listing = listing[jax.random.permutation(jax.random.fold_in(own, 1), rows)]
    offset_by = jax.random.randint(jax.random.fold_in(own, 2), (rows, 1), 0, top)
    return jnp.take_along_axis(listing, (jnp.arange(top)[None, :] + offset_by) % top, axis=1)


def load_shares(amount, total, most, lean, full):
    loads = [(1 << 20) // math.isqrt(grade ** lean) + 1 for grade in range(1, amount + 1)]
    largest = most if full else min(most, max(-(-total // amount), total * loads[0] // sum(loads)))
    least = 1 if total - largest >= amount - 1 else 0
    counts, spare = [largest] + [least] * (amount - 1), total - largest - least * (amount - 1)
    while spare > 0:
        candidates = [i for i in range(1, amount) if counts[i] < largest] or [i for i in range(1, amount) if counts[i] < most]
        pool, budget = sum([loads[i] for i in candidates]), spare
        for i in candidates:
            extra = min(most - counts[i], max(1, budget * loads[i] // pool), spare)
            counts[i] = counts[i] + extra
            spare = spare - extra
    return np.array(counts)


def scatter_about(own_key, shape, width, limit, shards=(), kind=jnp.bfloat16):
    values = width * jax.random.normal(own_key, shape, jnp.float32)
    if shards:
        values = values * levels(own_key, shape, shards, -0.22, 0.18)
    return jnp.clip(values, -limit, limit).astype(kind)


def setup_inputs(seed: int = 0) -> dict:
    splits = jax.random.split(jax.random.key(seed), 19)
    tokens = scatter_about(splits[0], (TOKENS, D), 1.0, 6.0, ((0, 64),))
    recur_state = scatter_about(splits[1], (TOKENS, H, HEAD, HEAD), 0.05, 0.4, ((0, 64), (1, 4)), jnp.float32)
    attn_gain = jnp.clip(1.0 + 0.18 * jax.random.normal(splits[2], (D,), jnp.float32), 0.1, 1.9)
    query_weight = scatter_about(splits[3], (D, H * HEAD), D ** -0.5, 0.125, ((1, 4),))
    key_weight = scatter_about(splits[4], (D, H * HEAD), D ** -0.5, 0.125, ((1, 4),))
    value_weight = scatter_about(splits[5], (D, H * HEAD), D ** -0.5, 0.125, ((1, 4),))
    outgate_weight = scatter_about(splits[6], (D, H * HEAD), D ** -0.5, 0.125, ((1, 4),))
    beta_weight = scatter_about(splits[7], (D, H), D ** -0.5, 0.125)
    decay_weight = scatter_about(splits[8], (D, H), D ** -0.5, 0.125)
    decay_rate = jnp.clip(jnp.exp(jax.random.uniform(splits[9], (H,), jnp.float32, math.log(0.05), math.log(2.0))), 0.05, 2.0)
    head_gain = jnp.clip(1.0 + 0.18 * jax.random.normal(splits[10], (HEAD,), jnp.float32), 0.1, 1.9)
    output_weight = scatter_about(splits[11], (H * HEAD, D), (H * HEAD) ** -0.5, 0.1875, ((0, 4),))
    ffn_gain = jnp.clip(1.0 + 0.18 * jax.random.normal(splits[12], (D,), jnp.float32), 0.1, 1.9)
    routes_keys = jax.random.split(jax.random.fold_in(splits[13], 1), TOKENS // SEQ_DEV)
    routes_turns = jax.random.permutation(jax.random.fold_in(splits[13], 3), TOKENS // SEQ_DEV)
    routes = jax.vmap(lambda own, number: shared_out(jax.random.fold_in(splits[13], 2), own, number, SEQ_DEV, EXPERTS, TOP, CAP, 2))(routes_keys, routes_turns).reshape((TOKENS, TOP))
    route_weight = jnp.clip(jnp.exp(math.log(1.0) - 1.609438 * jax.random.uniform(splits[14], (TOKENS, TOP), jnp.float32) ** levels(splits[14], (TOKENS, TOP), ((0, 64),), -0.2, 0.2)), 0.2, 1.0)
    expert_gate = scatter_about(splits[15], (4 * EXPERTS, D, FF_PART), D ** -0.5, 0.125, ((0, 64), (2, 4)))
    expert_up = scatter_about(splits[16], (4 * EXPERTS, D, FF_PART), D ** -0.5, 0.125, ((0, 64), (2, 4)))
    expert_down = scatter_about(splits[17], (4 * EXPERTS, FF_PART, D), FF_E ** -0.5, 0.09375, ((0, 64), (1, 4)))
    return {"tokens": tokens, "recur_state": recur_state, "attn_gain": attn_gain, "query_weight": query_weight, "key_weight": key_weight, "value_weight": value_weight, "outgate_weight": outgate_weight, "beta_weight": beta_weight, "decay_weight": decay_weight, "decay_rate": decay_rate, "head_gain": head_gain, "output_weight": output_weight, "ffn_gain": ffn_gain, "routes": routes, "route_weight": route_weight, "expert_gate": expert_gate, "expert_up": expert_up, "expert_down": expert_down}


EPS = 1e-06

def rms_scale(values, gain):
    return values * lax.rsqrt(lax.optimization_barrier(jnp.mean(values * values, axis=-1, keepdims=True)) + EPS) * gain

def unit_rows(values):
    return values * lax.rsqrt(lax.optimization_barrier(jnp.sum(values * values, axis=-1, keepdims=True)) + EPS)

def slot_targets(group_routes, experts, capacity):
    flat = group_routes.reshape(-1)
    onehot = (flat[:, None] == jnp.arange(experts, dtype=jnp.int32)[None, :]).astype(jnp.int32)
    running = jnp.cumsum(onehot, axis=0)
    position = lax.optimization_barrier(jnp.sum(running * onehot, axis=1)) - 1
    return (flat * capacity + position).reshape(group_routes.shape).astype(jnp.int32)

def reference(tokens, recur_state, attn_gain, query_weight, key_weight, value_weight, outgate_weight, beta_weight, decay_weight, decay_rate, head_gain, output_weight, ffn_gain, routes, route_weight, expert_gate, expert_up, expert_down):
    f32 = jnp.float32
    bf16 = jnp.bfloat16
    highest = lax.Precision.HIGHEST
    normed = rms_scale(tokens.astype(f32), attn_gain).astype(bf16)
    qproj = jnp.dot(normed, query_weight, preferred_element_type=f32).astype(bf16)
    kproj = jnp.dot(normed, key_weight, preferred_element_type=f32).astype(bf16)
    vproj = jnp.dot(normed, value_weight, preferred_element_type=f32).astype(bf16)
    zproj = jnp.dot(normed, outgate_weight, preferred_element_type=f32).astype(bf16)
    strength = jax.nn.sigmoid(jnp.dot(normed, beta_weight, preferred_element_type=f32))
    fading = jnp.exp(-decay_rate * jax.nn.softplus(jnp.dot(normed, decay_weight, preferred_element_type=f32)))

    def split_heads(proj):
        return proj.astype(f32).reshape(TOKENS, H, HEAD)
    query = unit_rows(jax.nn.silu(split_heads(qproj))) * HEAD ** (-0.5)
    keyvec = unit_rows(jax.nn.silu(split_heads(kproj)))
    value = jax.nn.silu(split_heads(vproj))
    recall = jnp.einsum('thd,thde->the', keyvec, recur_state, precision=highest)
    written = (strength[..., None] * keyvec)[..., :, None] * (value - fading[..., None] * recall)[..., None, :]
    new_state = fading[..., None, None] * recur_state + written
    readout = jnp.einsum('thd,thde->the', query, new_state, precision=highest)
    headed = (rms_scale(readout, head_gain) * jax.nn.silu(split_heads(zproj))).reshape(TOKENS, H * HEAD).astype(bf16)
    branch = jnp.dot(headed, output_weight, preferred_element_type=f32).astype(bf16)
    resid = (tokens.astype(f32) + branch.astype(f32)).astype(bf16)
    ffn_in = rms_scale(resid.astype(f32), ffn_gain).astype(bf16)
    grouped = ffn_in.reshape(N_EP, SEQ_DEV, D)
    group_routes = routes.reshape(N_EP, SEQ_DEV, TOP)
    group_weight = route_weight.reshape(N_EP, SEQ_DEV, TOP)
    targets = jax.vmap(lambda block: slot_targets(block, EXPERTS, CAP))(group_routes)
    slot_ids = jnp.arange(EXPERTS * CAP, dtype=jnp.int32)
    select = jnp.any(targets[:, None, :, :] == slot_ids[None, :, None, None], axis=-1).astype(f32)
    buffers = jnp.einsum('gst,gtd->gsd', select, grouped.astype(f32), precision=highest).astype(bf16)
    per_expert = buffers.reshape(N_EP, EXPERTS, CAP, D).transpose(1, 0, 2, 3).reshape(EXPERTS, N_EP * CAP, D)
    gates = expert_gate.reshape(EXPERTS, 4, D, FF_PART)
    ups = expert_up.reshape(EXPERTS, 4, D, FF_PART)
    downs = expert_down.reshape(EXPERTS, 4, FF_PART, D)

    def run_expert(operands):
        rows, gate_set, up_set, down_set = operands
        total = jnp.zeros((rows.shape[0], D), f32)
        for slice_idx in range(4):
            gated = jnp.dot(rows, gate_set[slice_idx], preferred_element_type=f32)
            lifted = jnp.dot(rows, up_set[slice_idx], preferred_element_type=f32)
            hidden = (jax.nn.silu(gated) * lifted).astype(bf16)
            piece = lax.optimization_barrier(jnp.dot(hidden, down_set[slice_idx], preferred_element_type=f32).astype(bf16))
            total = total + piece.astype(f32)
        return total
    results = lax.map(run_expert, (per_expert, gates, ups, downs))
    results = results.reshape(EXPERTS, N_EP, CAP, D).transpose(1, 0, 2, 3).reshape(N_EP, EXPERTS * CAP, D)
    combine = jnp.zeros((N_EP, SEQ_DEV, EXPERTS * CAP), f32)
    for choice_idx in range(TOP):
        match = (targets[..., choice_idx, None] == slot_ids).astype(f32)
        combine = combine + group_weight[..., choice_idx, None] * match
    moe = jnp.einsum('gts,gsd->gtd', combine, results, precision=highest).reshape(TOKENS, D)
    mixed = (resid.astype(f32) + moe).astype(bf16)
    return (mixed, new_state)
```

```python
import functools

import jax
import jax.numpy as jnp
from jax import lax
from jax.experimental import pallas as pl
from jax.experimental.pallas import tpu as pltpu
from jax.sharding import PartitionSpec as P

EPS = 1e-06
MESH = pl.DeviceIdType.MESH
F32 = jnp.float32
BF16 = jnp.bfloat16
CORES = 2
RING_Y = 4
CAP = 4
PARTS = 4
LANE = 128
TILE = CAP * PARTS
GROUPS = 4


def rms_scale(values, gain):
    return values * lax.rsqrt(jnp.mean(values * values, axis=-1, keepdims=True) + EPS) * gain


def unit_rows(values):
    return values * lax.rsqrt(jnp.sum(values * values, axis=-1, keepdims=True) + EPS)


def hop(slot, ring_z):
    i, dy = slot // RING_Y, slot % RING_Y
    dz = (i % 2) * ((i + 1) // 2) + (1 - i % 2) * ((ring_z - i // 2) % ring_z)
    return dz, dy


def iota(shape, dim):
    return lax.broadcasted_iota(jnp.int32, shape, dim)


def exchange_kernel(
    lanes, groups, partial_ref, tokens_ref, routes_ref, rw_ref, gain_ref, gate_hbm, up_hbm, down_hbm, out_ref,
    branch, packed, rows, wgate, wup, wdown, ysend, yrecv, gathered, back, resid_keep,
    local_sem, swap_send, swap_recv, b_send, b_recv, c_send, c_recv, d_send, d_recv, f_send, f_recv, g_send, g_recv,
):
    ring_z = groups // (RING_Y * CORES)
    plane = ring_z * RING_Y
    per_group = plane // GROUPS
    tp = lax.axis_index("tp")
    ep = lax.axis_index("ep")
    core = ep % CORES
    y = (ep // CORES) % RING_Y
    z = ep // (CORES * RING_Y)
    width = partial_ref.shape[1] // lanes

    def at(zz, yy):
        return (zz * RING_Y + yy) * CORES + core

    def forward(slot):
        dz, dy = hop(slot, ring_z)
        return (z + dz) % ring_z, (y + dy) % RING_Y

    def backward(slot):
        dz, dy = hop(slot, ring_z)
        return (z + ring_z - dz) % ring_z, (y + RING_Y - dy) % RING_Y

    partner = ep + 1 - 2 * core

    weights = ((gate_hbm, wgate), (up_hbm, wup), (down_hbm, wdown))
    loads = [pltpu.make_async_copy(src.at[0], dst.at[0], local_sem.at[i]) for i, (src, dst) in enumerate(weights)]
    for load in loads:
        load.start()

    barrier = pltpu.get_barrier_semaphore()
    pl.semaphore_signal(barrier, inc=1, device_id=(partner, tp), device_id_type=MESH)
    for dx in range(1, lanes):
        pl.semaphore_signal(barrier, inc=1, device_id=(ep, (tp + dx) % lanes), device_id_type=MESH)

    @pl.loop(1, plane)
    def _(slot):
        zz, yy = forward(slot)
        pl.semaphore_signal(barrier, inc=1, device_id=(at(zz, yy), tp), device_id_type=MESH)

    pl.semaphore_wait(barrier, plane - 1 + lanes - 1 + 1)

    sums = []
    for dx in range(1, lanes):
        to = (tp + dx) % lanes
        copy = pltpu.make_async_remote_copy(
            src_ref=partial_ref.at[:, pl.ds(pl.multiple_of(to * width, LANE), width)],
            dst_ref=branch.at[dx - 1],
            send_sem=b_send.at[dx - 1],
            recv_sem=b_recv.at[dx - 1],
            device_id=(ep, to),
            device_id_type=MESH,
        )
        copy.start()
        sums.append(copy)

    swaps = [
        pltpu.make_async_remote_copy(
            src_ref=src.at[0], dst_ref=dst.at[1], send_sem=swap_send.at[i], recv_sem=swap_recv.at[i],
            device_id=(partner, tp), device_id_type=MESH,
        )
        for i, (src, dst) in enumerate(weights)
    ]
    for swap in swaps:
        swap.start()

    experts = groups // 4
    seqs = routes_ref.shape[0]
    routes = routes_ref[...]
    rw = rw_ref[...]
    onehots = [(routes[:, k : k + 1] == iota((seqs, experts), 1)).astype(F32) for k in range(routes.shape[1])]
    earlier = (iota((seqs, seqs), 1) < iota((seqs, seqs), 0)).astype(F32)
    counts = jnp.dot(earlier, sum(onehots), preferred_element_type=F32)
    targets = []
    for k, onehot in enumerate(onehots):
        position = jnp.sum(counts * onehot, axis=1, keepdims=True).astype(jnp.int32)
        targets.append(routes[:, k : k + 1] * CAP + position)
    tall = [jnp.concatenate([t] * PARTS, axis=0) for t in targets]
    tall_w = [jnp.concatenate([rw[:, k : k + 1]] * PARTS, axis=0) for k in range(len(targets))]
    height = PARTS * seqs
    lane_id = iota((height, experts * TILE), 1)
    slot_of = (lane_id // TILE) * CAP + lane_id % CAP
    same_part = (lane_id % TILE) // CAP == iota((height, experts * TILE), 0) // seqs
    chosen = (tall[0] == slot_of) | (tall[1] == slot_of)
    select = (chosen & same_part).astype(F32).astype(BF16)

    mine = pl.ds(pl.multiple_of(tp * width, LANE), width)
    total = partial_ref[:, mine]
    for dx, copy in enumerate(sums):
        copy.wait_recv()
        total = total + branch[dx]
    resid = (tokens_ref[:, mine].astype(F32) + total.astype(BF16).astype(F32)).astype(BF16)
    resid_keep[...] = resid
    stacked = jnp.concatenate([resid[:, q * LANE : (q + 1) * LANE] for q in range(PARTS)], axis=0)
    picked = lax.dot_general(select, stacked, (((0,), (0,)), ((), ())), preferred_element_type=F32)
    packed[...] = picked.astype(BF16)

    def dispatch(slot):
        zz, yy = forward(slot)
        expert = zz * (RING_Y // 2) + yy // 2
        return pltpu.make_async_remote_copy(
            src_ref=packed.at[pl.ds(pl.multiple_of(expert * TILE, TILE), TILE), :],
            dst_ref=rows.at[tp, pl.ds(pl.multiple_of(slot * TILE, TILE), TILE), :],
            send_sem=c_send,
            recv_sem=c_recv.at[slot // per_group],
            device_id=(at(zz, yy), tp),
            device_id_type=MESH,
        )

    @pl.loop(1, plane)
    def _(slot):
        dispatch(slot).start()

    own_expert = z * (RING_Y // 2) + y // 2
    rows[tp, 0:TILE, :] = packed[pl.ds(pl.multiple_of(own_expert * TILE, TILE), TILE), :]

    def landed(ref, send_sem, recv_sem):
        return pltpu.make_async_remote_copy(
            src_ref=ref, dst_ref=ref, send_sem=send_sem, recv_sem=recv_sem, device_id=(partner, tp), device_id_type=MESH
        )

    spreads = []
    for g in range(GROUPS):
        first, last = g * per_group * TILE, (g + 1) * per_group * TILE
        fresh = max(first, TILE)
        landed(rows.at[tp, fresh:last, :], c_send, c_recv.at[g]).wait_recv()
        for dx in range(1, lanes):
            copy = pltpu.make_async_remote_copy(
                src_ref=rows.at[tp, first:last, :],
                dst_ref=rows.at[tp, first:last, :],
                send_sem=d_send.at[g, dx - 1],
                recv_sem=d_recv.at[g, dx - 1],
                device_id=(ep, (tp + dx) % lanes),
                device_id_type=MESH,
            )
            copy.start()
            spreads.append((g, dx, first, last, copy))

    lane_id = iota((height, plane * TILE), 1)
    dz, dy = hop(lane_id // TILE, ring_z)
    expert = ((z + dz) % ring_z) * (RING_Y // 2) + ((y + dy) % RING_Y) // 2
    slot_of = expert * CAP + lane_id % CAP
    same_part = (lane_id % TILE) // CAP == iota((height, plane * TILE), 0) // seqs
    combine = jnp.zeros((height, plane * TILE), F32)
    for target, weight in zip(tall, tall_w):
        combine = combine + jnp.where((target == slot_of) & same_part, weight, 0.0)

    many = 16
    span = many * TILE
    row_id, col_id = iota((span, span), 0), iota((span, span), 1)

    def shuffled(index):
        part, rest = index // (many * CAP), index % (many * CAP)
        return (rest // CAP) * TILE + part * CAP + rest % CAP

    sort = (shuffled(row_id) == col_id).astype(F32).astype(BF16)
    unsort = (shuffled(col_id) == row_id).astype(F32).astype(BF16)

    for g, dx, first, last, copy in spreads:
        source = (tp + lanes - dx) % lanes
        landed(rows.at[source, first:last, :], d_send.at[g, dx - 1], d_recv.at[g, dx - 1]).wait_recv()

    chunks = plane // many
    pieces = []
    for c in range(chunks):
        wide = jnp.concatenate([rows[x, c * span : (c + 1) * span, :] for x in range(lanes)], axis=1)
        ordered = jnp.dot(sort, wide, preferred_element_type=F32)
        high = many * CAP
        pieces.append(
            jnp.concatenate(
                [ordered[q * high : (q + 1) * high, x * LANE : (x + 1) * LANE] for x in range(lanes) for q in range(PARTS)],
                axis=1,
            )
        )
    arrived = jnp.concatenate(pieces, axis=0)
    ffn_in = rms_scale(arrived, gain_ref[...]).astype(BF16)

    for load in loads:
        load.wait()
    for swap in swaps:
        swap.wait_recv()
    hidden = []
    for s in range(CORES):
        gated = jnp.dot(ffn_in, wgate[s], preferred_element_type=F32)
        lifted = jnp.dot(ffn_in, wup[s], preferred_element_type=F32)
        hidden.append((jax.nn.silu(gated) * lifted).astype(BF16))

    gives = []
    high = many * CAP
    for c in range(chunks):
        part = sum(
            jnp.dot(hidden[s][c * high : (c + 1) * high], wdown[s], preferred_element_type=F32) for s in range(CORES)
        ).astype(BF16)
        tall_part = jnp.concatenate(
            [
                jnp.concatenate([part[:, (x * PARTS + q) * LANE : (x * PARTS + q + 1) * LANE] for x in range(lanes)], axis=1)
                for q in range(PARTS)
            ],
            axis=0,
        )
        split = jnp.dot(unsort, tall_part, preferred_element_type=F32).astype(BF16)
        for x in range(lanes):
            ysend[x, c * span : (c + 1) * span, :] = split[:, x * LANE : (x + 1) * LANE]
        for dx in range(1, lanes):
            to = (tp + dx) % lanes
            copy = pltpu.make_async_remote_copy(
                src_ref=ysend.at[to, c * span : (c + 1) * span, :],
                dst_ref=yrecv.at[dx - 1, c * span : (c + 1) * span, :],
                send_sem=f_send.at[c, dx - 1],
                recv_sem=f_recv.at[c, dx - 1],
                device_id=(ep, to),
                device_id_type=MESH,
            )
            copy.start()
            gives.append(copy)

    def give_back(slot):
        zz, yy = backward(slot)
        return pltpu.make_async_remote_copy(
            src_ref=gathered.at[pl.ds(pl.multiple_of(slot * TILE, TILE), TILE), :],
            dst_ref=back.at[pl.ds(pl.multiple_of(slot * TILE, TILE), TILE), :],
            send_sem=g_send,
            recv_sem=g_recv,
            device_id=(at(zz, yy), tp),
            device_id_type=MESH,
        )

    for c in range(chunks):
        own = ysend[tp, c * span : (c + 1) * span, :].astype(F32)
        for dx in range(1, lanes):
            gives[c * (lanes - 1) + dx - 1].wait_recv()
            own = own + yrecv[dx - 1, c * span : (c + 1) * span, :].astype(F32)
        gathered[c * span : (c + 1) * span, :] = own.astype(BF16)

        @pl.loop(max(1, c * many), (c + 1) * many)
        def _(slot):
            give_back(slot).start()

        if c == 0:
            back[0:TILE, :] = gathered[0:TILE, :]

    landed(back.at[TILE : plane * TILE, :], g_send, g_recv).wait_recv()
    moe = jnp.dot(combine, back[...].astype(F32), preferred_element_type=F32, precision=lax.Precision.HIGHEST)
    moe = jnp.concatenate([moe[q * seqs : (q + 1) * seqs] for q in range(PARTS)], axis=1)
    out_ref[...] = (resid_keep[...].astype(F32) + moe).astype(BF16)

    for copy in sums:
        copy.wait_send()
    for swap in swaps:
        swap.wait_send()
    landed(back.at[TILE : plane * TILE, :], c_send, g_recv).wait_send()
    for _, _, _, _, copy in spreads:
        copy.wait_send()
    for copy in gives:
        copy.wait_send()
    landed(back.at[TILE : plane * TILE, :], g_send, g_recv).wait_send()


def exchange(partial_out, tokens, routes, route_weight, ffn_gain, expert_gate, expert_up, expert_down):
    lanes, groups = lax.axis_size("tp"), lax.axis_size("ep")
    seqs, model = tokens.shape
    width = model // lanes
    plane = groups // CORES
    chunks = plane // 16
    hidden = expert_gate.shape[2]
    vmem, anywhere = pl.BlockSpec(memory_space=pltpu.VMEM), pl.BlockSpec(memory_space=pl.ANY)
    dma = pltpu.SemaphoreType.DMA
    return pl.pallas_call(
        functools.partial(exchange_kernel, lanes, groups),
        name="exchange",
        out_shape=jax.ShapeDtypeStruct((seqs, width), BF16),
        in_specs=[vmem] * 5 + [anywhere] * 3,
        out_specs=vmem,
        scratch_shapes=[
            pltpu.VMEM((lanes - 1, seqs, width), F32),
            pltpu.VMEM((groups // 4 * TILE, LANE), BF16),
            pltpu.VMEM((lanes, plane * TILE, LANE), BF16),
            pltpu.VMEM((CORES, model, hidden), BF16),
            pltpu.VMEM((CORES, model, hidden), BF16),
            pltpu.VMEM((CORES, hidden, model), BF16),
            pltpu.VMEM((lanes, plane * TILE, LANE), BF16),
            pltpu.VMEM((lanes - 1, plane * TILE, LANE), BF16),
            pltpu.VMEM((plane * TILE, LANE), BF16),
            pltpu.VMEM((plane * TILE, LANE), BF16),
            pltpu.VMEM((seqs, width), BF16),
            dma((3,)),
            dma((3,)),
            dma((3,)),
            dma((lanes - 1,)),
            dma((lanes - 1,)),
            dma,
            dma((GROUPS,)),
            dma((GROUPS, lanes - 1)),
            dma((GROUPS, lanes - 1)),
            dma((chunks, lanes - 1)),
            dma((chunks, lanes - 1)),
            dma,
            dma,
        ],
        compiler_params=pltpu.CompilerParams(
            collective_id=0, has_side_effects=True, vmem_limit_bytes=32 * 1024 * 1024
        ),
    )(partial_out, tokens, routes, route_weight, ffn_gain.reshape(1, -1), expert_gate, expert_up, expert_down)


def local(
    tokens,
    recur_state,
    attn_gain,
    query_weight,
    key_weight,
    value_weight,
    outgate_weight,
    beta_weight,
    decay_weight,
    decay_rate,
    head_gain,
    output_weight,
    ffn_gain,
    routes,
    route_weight,
    expert_gate,
    expert_up,
    expert_down,
):
    highest = lax.Precision.HIGHEST
    seq_count = tokens.shape[0]
    heads_here = recur_state.shape[1]
    head_size = recur_state.shape[2]
    lane_index = lax.axis_index("tp")
    normed = rms_scale(tokens.astype(F32), attn_gain).astype(BF16)
    qproj = jnp.dot(normed, query_weight, preferred_element_type=F32).astype(BF16)
    kproj = jnp.dot(normed, key_weight, preferred_element_type=F32).astype(BF16)
    vproj = jnp.dot(normed, value_weight, preferred_element_type=F32).astype(BF16)
    zproj = jnp.dot(normed, outgate_weight, preferred_element_type=F32).astype(BF16)
    first_head = lane_index * heads_here
    own_beta = lax.dynamic_slice_in_dim(beta_weight, first_head, heads_here, 1)
    own_decay = lax.dynamic_slice_in_dim(decay_weight, first_head, heads_here, 1)
    own_rate = lax.dynamic_slice_in_dim(decay_rate, first_head, heads_here, 0)
    strength = jax.nn.sigmoid(jnp.dot(normed, own_beta, preferred_element_type=F32))
    fading = jnp.exp(-own_rate * jax.nn.softplus(jnp.dot(normed, own_decay, preferred_element_type=F32)))

    def split_heads(proj):
        return proj.astype(F32).reshape(seq_count, heads_here, head_size)

    query = unit_rows(jax.nn.silu(split_heads(qproj))) * head_size ** (-0.5)
    keyvec = unit_rows(jax.nn.silu(split_heads(kproj)))
    value = jax.nn.silu(split_heads(vproj))
    recall = jnp.einsum("thd,thde->the", keyvec, recur_state, precision=highest)
    written = (strength[..., None] * keyvec)[..., :, None] * (value - fading[..., None] * recall)[..., None, :]
    new_state = fading[..., None, None] * recur_state + written
    readout = jnp.einsum("thd,thde->the", query, new_state, precision=highest)
    headed = (
        (rms_scale(readout, head_gain) * jax.nn.silu(split_heads(zproj)))
        .reshape(seq_count, heads_here * head_size)
        .astype(BF16)
    )
    partial_out = jnp.dot(headed, output_weight, preferred_element_type=F32)
    mixed = exchange(partial_out, tokens, routes, route_weight, ffn_gain, expert_gate, expert_up, expert_down)
    return (mixed, new_state)


def solution(mesh):
    return jax.shard_map(
        local,
        mesh=mesh,
        in_specs=(
            P("ep", None),
            P("ep", "tp", None, None),
            P(),
            P(None, "tp"),
            P(None, "tp"),
            P(None, "tp"),
            P(None, "tp"),
            P(),
            P(),
            P(),
            P(),
            P("tp", None),
            P(),
            P("ep", None),
            P("ep", None),
            P("ep", None, "tp"),
            P("ep", None, "tp"),
            P("ep", "tp", None),
        ),
        out_specs=(P("ep", "tp"), P("ep", "tp", None, None)),
        check_vma=False,
    )
```

```python
import functools

import jax
import jax.numpy as jnp
from jax import lax
from jax.experimental import pallas as pl
from jax.experimental.pallas import tpu as pltpu
from jax.sharding import PartitionSpec as P

EPS = 1e-06
MESH = pl.DeviceIdType.MESH
F32 = jnp.float32
BF16 = jnp.bfloat16
HIGHEST = lax.Precision.HIGHEST
CORES = 2
RING_Y = 4
CAP = 4
PARTS = 4
LANE = 128
TILE = CAP * PARTS
GROUPS = 4
STATE_CHUNKS = 4


def rms_scale(values, gain):
    return values * lax.rsqrt(jnp.mean(values * values, axis=-1, keepdims=True) + EPS) * gain


def unit_rows(values):
    return values * lax.rsqrt(jnp.sum(values * values, axis=-1, keepdims=True) + EPS)


def hop(slot, ring_z):
    i, dy = slot // RING_Y, slot % RING_Y
    dz = (i % 2) * ((i + 1) // 2) + (1 - i % 2) * ((ring_z - i // 2) % ring_z)
    return dz, dy


def iota(shape, dim):
    return lax.broadcasted_iota(jnp.int32, shape, dim)


def mixer_kernel(
    heads, tokens_ref, gain_ref, beta_ref, decay_ref, rate_ref, head_gain_ref, q_hbm, k_hbm, v_hbm, z_hbm, o_hbm, state_hbm,
    partial_ref, new_hbm, wq, wk, wv, wz, wo, state, read, load_sem, state_sem, out_sem,
):
    tp = lax.axis_index("tp")
    seqs = tokens_ref.shape[0]
    loads = {
        name: pltpu.make_async_copy(src, dst, load_sem.at[i])
        for i, (name, src, dst) in enumerate(
            (("k", k_hbm, wk), ("q", q_hbm, wq), ("v", v_hbm, wv), ("z", z_hbm, wz), ("o", o_hbm, wo))
        )
    }
    step = seqs // STATE_CHUNKS
    reads = [
        pltpu.make_async_copy(state_hbm.at[pl.ds(c * step, step)], state.at[pl.ds(c * step, step)], state_sem.at[c])
        for c in range(STATE_CHUNKS)
    ]
    for name in "kqv":
        loads[name].start()
    for read_in in reads:
        read_in.start()
    for name in "zo":
        loads[name].start()

    normed = rms_scale(tokens_ref[...].astype(F32), gain_ref[...]).astype(BF16)

    def by_head(weight_ref):
        return lax.dot_general(normed, weight_ref[...], (((1,), (1,)), ((), ())), preferred_element_type=F32)

    strength = jax.nn.sigmoid(by_head(beta_ref))
    fading = jnp.exp(-rate_ref[...] * jax.nn.softplus(by_head(decay_ref)))

    def own_head(values, h):
        chosen = iota(values.shape, 1) == tp * heads + h
        column = jnp.sum(jnp.where(chosen, values, 0.0), axis=1, keepdims=True)
        return jnp.broadcast_to(column, (seqs, LANE))

    strengths = [own_head(strength, h) for h in range(heads)]
    fadings = [own_head(fading, h) for h in range(heads)]

    def project(name, weight):
        loads[name].wait()
        proj = jnp.dot(normed, weight[...], preferred_element_type=F32).astype(BF16).astype(F32)
        return [jax.nn.silu(proj[:, h * LANE : (h + 1) * LANE]) for h in range(heads)]

    keys = [unit_rows(k) for k in project("k", wk)]
    queries = [unit_rows(q) * LANE ** (-0.5) for q in project("q", wq)]
    filler = [jnp.zeros((LANE - 2 * heads * seqs, LANE), F32)]
    columns = jnp.concatenate(keys + queries + filler, axis=0).T
    values = project("v", wv)

    writes = []
    for c in range(STATE_CHUNKS):
        reads[c].wait()
        for t in range(c * step, (c + 1) * step):
            for h in range(heads):
                j = h * seqs + t
                key, query = columns[:, j : j + 1], columns[:, heads * seqs + j : heads * seqs + j + 1]
                fade = fadings[h][t : t + 1]
                old = state[t, h]
                recall = jnp.sum(old * key, axis=0, keepdims=True)
                delta = strengths[h][t : t + 1] * (values[h][t : t + 1] - fade * recall)
                new = fade * old + key * delta
                state[t, h] = new
                read[t : t + 1, h * LANE : (h + 1) * LANE] = jnp.sum(new * query, axis=0, keepdims=True)
        write = pltpu.make_async_copy(state.at[pl.ds(c * step, step)], new_hbm.at[pl.ds(c * step, step)], out_sem.at[c])
        write.start()
        writes.append(write)

    gates = project("z", wz)
    headed = [
        (rms_scale(read[:, h * LANE : (h + 1) * LANE], head_gain_ref[...]) * gates[h]).astype(BF16) for h in range(heads)
    ]
    loads["o"].wait()
    partial_ref[...] = jnp.dot(jnp.concatenate(headed, axis=1), wo[...], preferred_element_type=F32)
    for write in writes:
        write.wait()


def mixer(
    tokens, recur_state, attn_gain, query_weight, key_weight, value_weight, outgate_weight, beta_weight, decay_weight,
    decay_rate, head_gain, output_weight,
):
    seqs, model = tokens.shape
    heads, size = recur_state.shape[1:3]
    vmem, anywhere = pl.BlockSpec(memory_space=pltpu.VMEM), pl.BlockSpec(memory_space=pltpu.HBM)
    dma = pltpu.SemaphoreType.DMA
    return pl.pallas_call(
        functools.partial(mixer_kernel, heads),
        name="mixer",
        out_shape=(jax.ShapeDtypeStruct((seqs, model), F32), jax.ShapeDtypeStruct(recur_state.shape, F32)),
        in_specs=[vmem] * 6 + [anywhere] * 6,
        out_specs=(vmem, anywhere),
        scratch_shapes=[pltpu.VMEM((model, heads * size), BF16)] * 4
        + [
            pltpu.VMEM((heads * size, model), BF16),
            pltpu.VMEM(recur_state.shape, F32),
            pltpu.VMEM((seqs, heads * size), F32),
            dma((5,)),
            dma((STATE_CHUNKS,)),
            dma((STATE_CHUNKS,)),
        ],
        compiler_params=pltpu.CompilerParams(vmem_limit_bytes=24 * 1024 * 1024),
    )(
        tokens, attn_gain.reshape(1, -1), beta_weight.T, decay_weight.T, decay_rate.reshape(1, -1), head_gain.reshape(1, -1),
        query_weight, key_weight, value_weight, outgate_weight, output_weight, recur_state,
    )


def exchange_kernel(
    lanes, groups, partial_ref, tokens_ref, routes_ref, rw_ref, gain_ref, gate_hbm, up_hbm, down_hbm, out_ref,
    branch, packed, rows, wgate, wup, wdown, ysend, yrecv, gathered, back, resid_keep,
    local_sem, swap_send, swap_recv, b_send, b_recv, c_send, c_recv, d_send, d_recv, f_send, f_recv, g_send, g_recv,
):
    ring_z = groups // (RING_Y * CORES)
    plane = ring_z * RING_Y
    per_group = plane // GROUPS
    tp = lax.axis_index("tp")
    ep = lax.axis_index("ep")
    core = ep % CORES
    y = (ep // CORES) % RING_Y
    z = ep // (CORES * RING_Y)
    width = partial_ref.shape[1] // lanes

    def at(zz, yy):
        return (zz * RING_Y + yy) * CORES + core

    def forward(slot):
        dz, dy = hop(slot, ring_z)
        return (z + dz) % ring_z, (y + dy) % RING_Y

    def backward(slot):
        dz, dy = hop(slot, ring_z)
        return (z + ring_z - dz) % ring_z, (y + RING_Y - dy) % RING_Y

    partner = ep + 1 - 2 * core

    weights = ((gate_hbm, wgate), (up_hbm, wup), (down_hbm, wdown))
    loads = [pltpu.make_async_copy(src.at[0], dst.at[0], local_sem.at[i]) for i, (src, dst) in enumerate(weights)]
    for load in loads:
        load.start()

    barrier = pltpu.get_barrier_semaphore()
    pl.semaphore_signal(barrier, inc=1, device_id=(partner, tp), device_id_type=MESH)
    for dx in range(1, lanes):
        pl.semaphore_signal(barrier, inc=1, device_id=(ep, (tp + dx) % lanes), device_id_type=MESH)

    @pl.loop(1, plane)
    def _(slot):
        zz, yy = forward(slot)
        pl.semaphore_signal(barrier, inc=1, device_id=(at(zz, yy), tp), device_id_type=MESH)

    pl.semaphore_wait(barrier, plane - 1 + lanes - 1 + 1)

    sums = []
    for dx in range(1, lanes):
        to = (tp + dx) % lanes
        copy = pltpu.make_async_remote_copy(
            src_ref=partial_ref.at[:, pl.ds(pl.multiple_of(to * width, LANE), width)],
            dst_ref=branch.at[dx - 1],
            send_sem=b_send.at[dx - 1],
            recv_sem=b_recv.at[dx - 1],
            device_id=(ep, to),
            device_id_type=MESH,
        )
        copy.start()
        sums.append(copy)

    swaps = [
        pltpu.make_async_remote_copy(
            src_ref=src.at[0], dst_ref=dst.at[1], send_sem=swap_send.at[i], recv_sem=swap_recv.at[i],
            device_id=(partner, tp), device_id_type=MESH,
        )
        for i, (src, dst) in enumerate(weights)
    ]
    for swap in swaps:
        swap.start()

    experts = groups // 4
    seqs = routes_ref.shape[1]
    eye = (iota((seqs, seqs), 0) == iota((seqs, seqs), 1)).astype(F32)

    def upright(flat):
        return lax.dot_general(eye, flat, (((1,), (1,)), ((), ())), preferred_element_type=F32, precision=HIGHEST)

    routes = upright(routes_ref[...].astype(F32)).astype(jnp.int32)
    rw = upright(rw_ref[...])
    onehots = [(routes[:, k : k + 1] == iota((seqs, experts), 1)).astype(F32) for k in range(routes.shape[1])]
    earlier = (iota((seqs, seqs), 1) < iota((seqs, seqs), 0)).astype(F32)
    counts = jnp.dot(earlier, sum(onehots), preferred_element_type=F32)
    targets = []
    for k, onehot in enumerate(onehots):
        position = jnp.sum(counts * onehot, axis=1, keepdims=True).astype(jnp.int32)
        targets.append(routes[:, k : k + 1] * CAP + position)
    tall = [jnp.concatenate([t] * PARTS, axis=0) for t in targets]
    tall_w = [jnp.concatenate([rw[:, k : k + 1]] * PARTS, axis=0) for k in range(len(targets))]
    height = PARTS * seqs
    lane_id = iota((height, experts * TILE), 1)
    slot_of = (lane_id // TILE) * CAP + lane_id % CAP
    same_part = (lane_id % TILE) // CAP == iota((height, experts * TILE), 0) // seqs
    chosen = (tall[0] == slot_of) | (tall[1] == slot_of)
    select = (chosen & same_part).astype(F32).astype(BF16)

    mine = pl.ds(pl.multiple_of(tp * width, LANE), width)
    total = partial_ref[:, mine]
    for dx, copy in enumerate(sums):
        copy.wait_recv()
        total = total + branch[dx]
    resid = (tokens_ref[:, mine].astype(F32) + total.astype(BF16).astype(F32)).astype(BF16)
    resid_keep[...] = resid
    stacked = jnp.concatenate([resid[:, q * LANE : (q + 1) * LANE] for q in range(PARTS)], axis=0)
    picked = lax.dot_general(select, stacked, (((0,), (0,)), ((), ())), preferred_element_type=F32)
    packed[...] = picked.astype(BF16)

    def dispatch(slot):
        zz, yy = forward(slot)
        expert = zz * (RING_Y // 2) + yy // 2
        return pltpu.make_async_remote_copy(
            src_ref=packed.at[pl.ds(pl.multiple_of(expert * TILE, TILE), TILE), :],
            dst_ref=rows.at[tp, pl.ds(pl.multiple_of(slot * TILE, TILE), TILE), :],
            send_sem=c_send,
            recv_sem=c_recv.at[slot // per_group],
            device_id=(at(zz, yy), tp),
            device_id_type=MESH,
        )

    @pl.loop(1, plane)
    def _(slot):
        dispatch(slot).start()

    own_expert = z * (RING_Y // 2) + y // 2
    rows[tp, 0:TILE, :] = packed[pl.ds(pl.multiple_of(own_expert * TILE, TILE), TILE), :]

    def landed(ref, send_sem, recv_sem):
        return pltpu.make_async_remote_copy(
            src_ref=ref, dst_ref=ref, send_sem=send_sem, recv_sem=recv_sem, device_id=(partner, tp), device_id_type=MESH
        )

    spreads = []
    for g in range(GROUPS):
        first, last = g * per_group * TILE, (g + 1) * per_group * TILE
        fresh = max(first, TILE)
        landed(rows.at[tp, fresh:last, :], c_send, c_recv.at[g]).wait_recv()
        for dx in range(1, lanes):
            copy = pltpu.make_async_remote_copy(
                src_ref=rows.at[tp, first:last, :],
                dst_ref=rows.at[tp, first:last, :],
                send_sem=d_send.at[g, dx - 1],
                recv_sem=d_recv.at[g, dx - 1],
                device_id=(ep, (tp + dx) % lanes),
                device_id_type=MESH,
            )
            copy.start()
            spreads.append((g, dx, first, last, copy))

    lane_id = iota((height, plane * TILE), 1)
    dz, dy = hop(lane_id // TILE, ring_z)
    expert = ((z + dz) % ring_z) * (RING_Y // 2) + ((y + dy) % RING_Y) // 2
    slot_of = expert * CAP + lane_id % CAP
    same_part = (lane_id % TILE) // CAP == iota((height, plane * TILE), 0) // seqs
    combine = jnp.zeros((height, plane * TILE), F32)
    for target, weight in zip(tall, tall_w):
        combine = combine + jnp.where((target == slot_of) & same_part, weight, 0.0)

    many = 16
    span = many * TILE
    row_id, col_id = iota((span, span), 0), iota((span, span), 1)

    def shuffled(index):
        part, rest = index // (many * CAP), index % (many * CAP)
        return (rest // CAP) * TILE + part * CAP + rest % CAP

    sort = (shuffled(row_id) == col_id).astype(F32).astype(BF16)
    unsort = (shuffled(col_id) == row_id).astype(F32).astype(BF16)

    for g, dx, first, last, copy in spreads:
        source = (tp + lanes - dx) % lanes
        landed(rows.at[source, first:last, :], d_send.at[g, dx - 1], d_recv.at[g, dx - 1]).wait_recv()

    chunks = plane // many
    pieces = []
    for c in range(chunks):
        wide = jnp.concatenate([rows[x, c * span : (c + 1) * span, :] for x in range(lanes)], axis=1)
        ordered = jnp.dot(sort, wide, preferred_element_type=F32)
        high = many * CAP
        pieces.append(
            jnp.concatenate(
                [ordered[q * high : (q + 1) * high, x * LANE : (x + 1) * LANE] for x in range(lanes) for q in range(PARTS)],
                axis=1,
            )
        )
    arrived = jnp.concatenate(pieces, axis=0)
    ffn_in = rms_scale(arrived, gain_ref[...]).astype(BF16)

    for load in loads:
        load.wait()
    for swap in swaps:
        swap.wait_recv()
    hidden = []
    for s in range(CORES):
        gated = jnp.dot(ffn_in, wgate[s], preferred_element_type=F32)
        lifted = jnp.dot(ffn_in, wup[s], preferred_element_type=F32)
        hidden.append((jax.nn.silu(gated) * lifted).astype(BF16))

    gives = []
    high = many * CAP
    for c in range(chunks):
        part = sum(
            jnp.dot(hidden[s][c * high : (c + 1) * high], wdown[s], preferred_element_type=F32) for s in range(CORES)
        ).astype(BF16)
        tall_part = jnp.concatenate(
            [
                jnp.concatenate([part[:, (x * PARTS + q) * LANE : (x * PARTS + q + 1) * LANE] for x in range(lanes)], axis=1)
                for q in range(PARTS)
            ],
            axis=0,
        )
        split = jnp.dot(unsort, tall_part, preferred_element_type=F32).astype(BF16)
        for x in range(lanes):
            ysend[x, c * span : (c + 1) * span, :] = split[:, x * LANE : (x + 1) * LANE]
        for dx in range(1, lanes):
            to = (tp + dx) % lanes
            copy = pltpu.make_async_remote_copy(
                src_ref=ysend.at[to, c * span : (c + 1) * span, :],
                dst_ref=yrecv.at[dx - 1, c * span : (c + 1) * span, :],
                send_sem=f_send.at[c, dx - 1],
                recv_sem=f_recv.at[c, dx - 1],
                device_id=(ep, to),
                device_id_type=MESH,
            )
            copy.start()
            gives.append(copy)

    def give_back(slot):
        zz, yy = backward(slot)
        return pltpu.make_async_remote_copy(
            src_ref=gathered.at[pl.ds(pl.multiple_of(slot * TILE, TILE), TILE), :],
            dst_ref=back.at[pl.ds(pl.multiple_of(slot * TILE, TILE), TILE), :],
            send_sem=g_send,
            recv_sem=g_recv,
            device_id=(at(zz, yy), tp),
            device_id_type=MESH,
        )

    for c in range(chunks):
        own = ysend[tp, c * span : (c + 1) * span, :].astype(F32)
        for dx in range(1, lanes):
            gives[c * (lanes - 1) + dx - 1].wait_recv()
            own = own + yrecv[dx - 1, c * span : (c + 1) * span, :].astype(F32)
        gathered[c * span : (c + 1) * span, :] = own.astype(BF16)

        @pl.loop(max(1, c * many), (c + 1) * many)
        def _(slot):
            give_back(slot).start()

        if c == 0:
            back[0:TILE, :] = gathered[0:TILE, :]

    landed(back.at[TILE : plane * TILE, :], g_send, g_recv).wait_recv()
    moe = jnp.dot(combine, back[...].astype(F32), preferred_element_type=F32, precision=HIGHEST)
    moe = jnp.concatenate([moe[q * seqs : (q + 1) * seqs] for q in range(PARTS)], axis=1)
    out_ref[...] = (resid_keep[...].astype(F32) + moe).astype(BF16)

    for copy in sums:
        copy.wait_send()
    for swap in swaps:
        swap.wait_send()
    landed(back.at[TILE : plane * TILE, :], c_send, g_recv).wait_send()
    for _, _, _, _, copy in spreads:
        copy.wait_send()
    for copy in gives:
        copy.wait_send()
    landed(back.at[TILE : plane * TILE, :], g_send, g_recv).wait_send()


def exchange(partial_out, tokens, routes, route_weight, ffn_gain, expert_gate, expert_up, expert_down):
    lanes, groups = lax.axis_size("tp"), lax.axis_size("ep")
    seqs, model = tokens.shape
    width = model // lanes
    plane = groups // CORES
    chunks = plane // 16
    hidden = expert_gate.shape[2]
    vmem, anywhere = pl.BlockSpec(memory_space=pltpu.VMEM), pl.BlockSpec(memory_space=pltpu.HBM)
    dma = pltpu.SemaphoreType.DMA
    return pl.pallas_call(
        functools.partial(exchange_kernel, lanes, groups),
        name="exchange",
        out_shape=jax.ShapeDtypeStruct((seqs, width), BF16),
        in_specs=[vmem] * 5 + [anywhere] * 3,
        out_specs=vmem,
        scratch_shapes=[
            pltpu.VMEM((lanes - 1, seqs, width), F32),
            pltpu.VMEM((groups // 4 * TILE, LANE), BF16),
            pltpu.VMEM((lanes, plane * TILE, LANE), BF16),
            pltpu.VMEM((CORES, model, hidden), BF16),
            pltpu.VMEM((CORES, model, hidden), BF16),
            pltpu.VMEM((CORES, hidden, model), BF16),
            pltpu.VMEM((lanes, plane * TILE, LANE), BF16),
            pltpu.VMEM((lanes - 1, plane * TILE, LANE), BF16),
            pltpu.VMEM((plane * TILE, LANE), BF16),
            pltpu.VMEM((plane * TILE, LANE), BF16),
            pltpu.VMEM((seqs, width), BF16),
            dma((3,)),
            dma((3,)),
            dma((3,)),
            dma((lanes - 1,)),
            dma((lanes - 1,)),
            dma,
            dma((GROUPS,)),
            dma((GROUPS, lanes - 1)),
            dma((GROUPS, lanes - 1)),
            dma((chunks, lanes - 1)),
            dma((chunks, lanes - 1)),
            dma,
            dma,
        ],
        compiler_params=pltpu.CompilerParams(
            collective_id=0, has_side_effects=True, vmem_limit_bytes=32 * 1024 * 1024
        ),
    )(partial_out, tokens, routes.T, route_weight.T, ffn_gain.reshape(1, -1), expert_gate, expert_up, expert_down)


def local(
    tokens,
    recur_state,
    attn_gain,
    query_weight,
    key_weight,
    value_weight,
    outgate_weight,
    beta_weight,
    decay_weight,
    decay_rate,
    head_gain,
    output_weight,
    ffn_gain,
    routes,
    route_weight,
    expert_gate,
    expert_up,
    expert_down,
):
    partial_out, new_state = mixer(
        tokens, recur_state, attn_gain, query_weight, key_weight, value_weight, outgate_weight, beta_weight, decay_weight,
        decay_rate, head_gain, output_weight,
    )
    mixed = exchange(partial_out, tokens, routes, route_weight, ffn_gain, expert_gate, expert_up, expert_down)
    return (mixed, new_state)


def solution(mesh):
    return jax.shard_map(
        local,
        mesh=mesh,
        in_specs=(
            P("ep", None),
            P("ep", "tp", None, None),
            P(),
            P(None, "tp"),
            P(None, "tp"),
            P(None, "tp"),
            P(None, "tp"),
            P(),
            P(),
            P(),
            P(),
            P("tp", None),
            P(),
            P("ep", None),
            P("ep", None),
            P("ep", None, "tp"),
            P("ep", None, "tp"),
            P("ep", "tp", None),
        ),
        out_specs=(P("ep", "tp"), P("ep", "tp", None, None)),
        check_vma=False,
    )
```

```python
import functools

import jax
import jax.numpy as jnp
from jax import lax
from jax.experimental import pallas as pl
from jax.experimental.pallas import tpu as pltpu
from jax.sharding import PartitionSpec as P

EPS = 1e-06
MESH = pl.DeviceIdType.MESH
F32 = jnp.float32
BF16 = jnp.bfloat16
HIGHEST = lax.Precision.HIGHEST
CORES = 2
RING_Y = 4
CAP = 4
PARTS = 4
LANE = 128
TILE = CAP * PARTS
GROUPS = 8
CHUNKS = ((0, 16), (16, 32))
PIECES = (((0, 16),), ((24, 32), (16, 24)))
STATE_CHUNKS = 4
VMEM_GRANT = 63 * 1024 * 1024
EXCHANGE_GRANT = 53 * 1024 * 1024


def rms_scale(values, gain):
    return values * lax.rsqrt(jnp.mean(values * values, axis=-1, keepdims=True) + EPS) * gain


def unit_rows(values):
    return values * lax.rsqrt(jnp.sum(values * values, axis=-1, keepdims=True) + EPS)


def hop(slot, ring_z):
    i, dy = slot // RING_Y, slot % RING_Y
    dz = (i % 2) * ((i + 1) // 2) + (1 - i % 2) * ((ring_z - i // 2) % ring_z)
    return dz, dy


def iota(shape, dim):
    return lax.broadcasted_iota(jnp.int32, shape, dim)


def fetch(pairs, sems):
    copies = [pltpu.make_async_copy(src, dst, sems.at[i]) for i, (src, dst) in enumerate(pairs)]
    for copy in copies:
        copy.start()
    return copies


def heads_of(proj):
    proj = proj.astype(BF16).astype(F32)
    return [jax.nn.silu(proj[:, at : at + LANE]) for at in range(0, proj.shape[1], LANE)]


def mixer_kernel(
    heads, tokens_hbm, gain_hbm, beta_hbm, decay_hbm, rate_hbm, k_hbm, q_hbm, v_hbm, state_hbm,
    read_hbm, new_hbm, tokens, gain, beta, decay, rate, wk, wq, wv, state, read, small_sem, load_sem, state_sem, out_sem,
    read_sem,
):
    tp = lax.axis_index("tp")
    seqs = tokens.shape[0]
    step = seqs // STATE_CHUNKS

    small = fetch(
        ((tokens_hbm, tokens), (gain_hbm, gain), (beta_hbm, beta), (decay_hbm, decay), (rate_hbm, rate)), small_sem
    )
    loads = fetch(((k_hbm, wk), (q_hbm, wq), (v_hbm, wv)), load_sem)
    parts = [pl.ds(c * step, step) for c in range(STATE_CHUNKS)]

    for copy in small + loads:
        copy.wait()
    reads = fetch([(state_hbm.at[part], state.at[part]) for part in parts], state_sem)
    normed = rms_scale(tokens[...].astype(F32), gain[...]).astype(BF16)

    def project(weight):
        return heads_of(jnp.dot(normed, weight[...], preferred_element_type=F32))

    keys = [unit_rows(k) for k in project(wk)]
    queries = [unit_rows(q) * LANE ** (-0.5) for q in project(wq)]
    values = project(wv)
    filler = [jnp.zeros((LANE - 2 * heads * seqs, LANE), F32)]
    columns = jnp.concatenate(keys + queries + filler, axis=0).T

    def by_head(weight):
        return lax.dot_general(normed, weight[...], (((1,), (1,)), ((), ())), preferred_element_type=F32)

    strength = jax.nn.sigmoid(by_head(beta))
    fading = jnp.exp(-rate[...] * jax.nn.softplus(by_head(decay)))

    def own_head(values, h):
        chosen = iota(values.shape, 1) == tp * heads + h
        column = jnp.sum(jnp.where(chosen, values, 0.0), axis=1, keepdims=True)
        return jnp.broadcast_to(column, (seqs, LANE))

    strengths = [own_head(strength, h) for h in range(heads)]
    fadings = [own_head(fading, h) for h in range(heads)]

    writes = []
    for c, part in enumerate(parts):
        reads[c].wait()
        for t in range(c * step, (c + 1) * step):
            for h in range(heads):
                j = h * seqs + t
                key, query = columns[:, j : j + 1], columns[:, heads * seqs + j : heads * seqs + j + 1]
                fade = fadings[h][t : t + 1]
                old = state[t, h]
                recall = jnp.sum(old * key, axis=0, keepdims=True)
                delta = strengths[h][t : t + 1] * (values[h][t : t + 1] - fade * recall)
                new = fade * old + key * delta
                state[t, h] = new
                read[t : t + 1, h * LANE : (h + 1) * LANE] = jnp.sum(new * query, axis=0, keepdims=True)
        write = pltpu.make_async_copy(state.at[part], new_hbm.at[part], out_sem.at[c])
        write.start()
        writes.append(write)
    write = pltpu.make_async_copy(read, read_hbm.at[0:seqs], read_sem)
    write.start()
    write.wait()
    for write in writes:
        write.wait()


def mixer(
    tokens, recur_state, attn_gain, query_weight, key_weight, value_weight, beta_weight, decay_weight, decay_rate
):
    seqs, model = tokens.shape
    heads, size = recur_state.shape[1:3]
    anywhere = pl.BlockSpec(memory_space=pltpu.HBM)
    dma = pltpu.SemaphoreType.DMA
    small = (tokens, attn_gain.reshape(1, -1), beta_weight.T, decay_weight.T, decay_rate.reshape(1, -1))
    return pl.pallas_call(
        functools.partial(mixer_kernel, heads),
        name="mixer",
        out_shape=(
            jax.ShapeDtypeStruct((model, heads * size), F32),
            jax.ShapeDtypeStruct(recur_state.shape, F32),
        ),
        in_specs=[anywhere] * 9,
        out_specs=(anywhere, anywhere),
        scratch_shapes=[pltpu.VMEM(array.shape, array.dtype) for array in small]
        + [pltpu.VMEM((model, heads * size), BF16)] * 3
        + [
            pltpu.VMEM(recur_state.shape, F32),
            pltpu.VMEM((seqs, heads * size), F32),
            dma((5,)),
            dma((3,)),
            dma((STATE_CHUNKS,)),
            dma((STATE_CHUNKS,)),
            dma,
        ],
        compiler_params=pltpu.CompilerParams(vmem_limit_bytes=VMEM_GRANT),
    )(*small, key_weight, query_weight, value_weight, recur_state)


def exchange_kernel(
    lanes, groups, tokens, attn_gain, head_gain, ffn_gain, routes_flat, rw_flat,
    read_hbm, z_hbm, o_hbm, gate_hbm, up_hbm, down_hbm, out_ref,
    read, wz, wo,
    partial, branch, packed, rows, wide_in, wdown, ysend, yrecv, gathered, back,
    ready, head_sem, local_sem, swap_send, swap_recv, b_send, b_recv, c_send, c_recv, d_send, d_recv,
    f_send, f_recv, g_send, g_recv,
):
    ring_z = groups // (RING_Y * CORES)
    plane = ring_z * RING_Y
    per_group = plane // GROUPS
    tp = lax.axis_index("tp")
    ep = lax.axis_index("ep")
    core = ep % CORES
    y = (ep // CORES) % RING_Y
    z = ep // (CORES * RING_Y)
    seqs, width = tokens.shape[0], tokens.shape[1] // lanes

    zs = [(z + dz) % ring_z for dz in range(ring_z)]
    ys = [(y + dy) % RING_Y for dy in range(RING_Y)]
    z_part = [zz * (RING_Y * CORES) for zz in zs]
    y_part = [yy * CORES + core for yy in ys]

    def forward(slot):
        dz, dy = hop(slot, ring_z)
        return z_part[dz] + y_part[dy]

    def backward(slot):
        dz, dy = hop(slot, ring_z)
        return z_part[-dz % ring_z] + y_part[-dy % RING_Y]

    partner = ep + 1 - 2 * core
    nearest_last = list(range(plane - 1, 0, -1))

    z_in, read_in, o_in = fetch(((z_hbm, wz), (read_hbm.at[0:seqs], read), (o_hbm, wo)), head_sem)

    barrier = pltpu.get_barrier_semaphore()
    for slot in nearest_last:
        pl.semaphore_signal(barrier, inc=1, device_id=(forward(slot), tp), device_id_type=MESH)
    for dx in range(1, lanes):
        pl.semaphore_signal(barrier, inc=1, device_id=(ep, (tp + dx) % lanes), device_id_type=MESH)

    @pl.when(core == 0)
    def _():
        pl.semaphore_signal(barrier, inc=1, device_id=(partner, tp), device_id_type=MESH)

    hidden = gate_hbm.shape[2]

    def weights(s):
        return (
            (gate_hbm.at[0], wide_in.at[s, :, 0:hidden]),
            (up_hbm.at[0], wide_in.at[s, :, hidden : 2 * hidden]),
            (down_hbm.at[0], wdown.at[s * hidden : (s + 1) * hidden, :]),
        )

    loads = fetch(weights(0), local_sem)

    normed = rms_scale(tokens[...].astype(F32), attn_gain[...]).astype(BF16)
    z_in.wait()
    read_in.wait()
    gates = heads_of(jnp.dot(normed, wz[...], preferred_element_type=F32))
    headed = [
        (rms_scale(read[:, h * LANE : (h + 1) * LANE], head_gain[...]) * gate).astype(BF16) for h, gate in enumerate(gates)
    ]
    o_in.wait()
    shares = jnp.dot(jnp.concatenate(headed, axis=1), wo[...], preferred_element_type=F32)
    partial[...] = shares.astype(BF16)

    pl.semaphore_wait(barrier, plane - 1 + lanes - 1 + core)

    sums = []
    for dx in range(1, lanes):
        to = (tp + dx) % lanes
        copy = pltpu.make_async_remote_copy(
            src_ref=partial.at[:, pl.ds(pl.multiple_of(to * width, LANE), width)],
            dst_ref=branch.at[dx - 1],
            send_sem=b_send.at[dx - 1],
            recv_sem=b_recv.at[dx - 1],
            device_id=(ep, to),
            device_id_type=MESH,
        )
        copy.start()
        sums.append(copy)

    swaps = [
        pltpu.make_async_remote_copy(
            src_ref=src, dst_ref=dst, send_sem=swap_send.at[i], recv_sem=swap_recv.at[i],
            device_id=(partner, tp), device_id_type=MESH,
        )
        for i, (src, dst) in enumerate(weights(1))
    ]

    @pl.when(core == 1)
    def _():
        pl.semaphore_signal(ready, inc=1, device_id=(partner, tp), device_id_type=MESH)
        for swap in swaps:
            swap.start()

    experts = groups // 4
    eye = (iota((seqs, seqs), 0) == iota((seqs, seqs), 1)).astype(F32)

    def upright(flat):
        return lax.dot_general(eye, flat, (((1,), (1,)), ((), ())), preferred_element_type=F32, precision=HIGHEST)

    routes = upright(routes_flat[...].astype(F32)).astype(jnp.int32)
    rw = upright(rw_flat[...])
    onehots = [(routes[:, k : k + 1] == iota((seqs, experts), 1)).astype(F32) for k in range(routes.shape[1])]
    earlier = (iota((seqs, seqs), 1) < iota((seqs, seqs), 0)).astype(F32)
    counts = jnp.dot(earlier, sum(onehots), preferred_element_type=F32)
    targets = []
    for k, onehot in enumerate(onehots):
        position = jnp.sum(counts * onehot, axis=1, keepdims=True).astype(jnp.int32)
        targets.append(routes[:, k : k + 1] * CAP + position)
    tall = [jnp.concatenate([t] * PARTS, axis=0) for t in targets]
    tall_w = [jnp.concatenate([rw[:, k : k + 1]] * PARTS, axis=0) for k in range(len(targets))]
    height = PARTS * seqs
    lane_id = iota((height, experts * TILE), 1)
    slot_of = (lane_id // TILE) * CAP + lane_id % CAP
    same_part = (lane_id % TILE) // CAP == iota((height, experts * TILE), 0) // seqs
    chosen = (tall[0] == slot_of) | (tall[1] == slot_of)
    select = (chosen & same_part).astype(F32).astype(BF16)

    mine = pl.ds(pl.multiple_of(tp * width, LANE), width)
    total = partial[:, mine].astype(F32)
    for dx, copy in enumerate(sums):
        copy.wait_recv()
        total = total + branch[dx].astype(F32)
    resid = (tokens[:, mine].astype(F32) + total.astype(BF16).astype(F32)).astype(BF16)
    stacked = jnp.concatenate([resid[:, q * LANE : (q + 1) * LANE] for q in range(PARTS)], axis=0)
    picked = lax.dot_general(select, stacked, (((0,), (0,)), ((), ())), preferred_element_type=F32)
    packed[...] = picked.astype(BF16)

    z_rows = [zz * (RING_Y // 2 * TILE) for zz in zs]
    y_rows = [yy // 2 * TILE for yy in ys]
    for slot in range(1, plane):
        dz, dy = hop(slot, ring_z)
        pltpu.make_async_remote_copy(
            src_ref=packed.at[pl.ds(pl.multiple_of(z_rows[dz] + y_rows[dy], TILE), TILE), :],
            dst_ref=rows.at[tp, slot * TILE : (slot + 1) * TILE, :],
            send_sem=c_send,
            recv_sem=c_recv.at[slot // per_group],
            device_id=(forward(slot), tp),
            device_id_type=MESH,
        ).start()

    rows[tp, 0:TILE, :] = packed[pl.ds(pl.multiple_of(z_rows[0] + y_rows[0], TILE), TILE), :]

    @pl.when(core == 0)
    def _():
        pl.semaphore_wait(ready, 1)
        for swap in swaps:
            swap.start()

    def landed(ref, send_sem, recv_sem):
        return pltpu.make_async_remote_copy(
            src_ref=ref, dst_ref=ref, send_sem=send_sem, recv_sem=recv_sem, device_id=(partner, tp), device_id_type=MESH
        )

    def shuffle(slots):
        high = slots * CAP
        shape = (slots * TILE, slots * TILE)

        def hit(dim):
            index = iota(shape, dim)
            part = sum((index >= q * high).astype(jnp.int32) for q in range(1, PARTS))
            rest = index - part * high
            return ((rest // CAP) * TILE + part * CAP + rest % CAP == iota(shape, 1 - dim)).astype(F32).astype(BF16)

        return hit(0), hit(1)

    shuffles = [shuffle(last - first) for first, last in CHUNKS]

    spreads = [[] for _ in CHUNKS]
    for g in range(GROUPS):
        first, last = g * per_group * TILE, (g + 1) * per_group * TILE
        fresh = max(first, TILE)
        landed(rows.at[tp, fresh:last, :], c_send, c_recv.at[g]).wait_recv()
        for dx in range(1, lanes):
            copy = pltpu.make_async_remote_copy(
                src_ref=rows.at[tp, first:last, :],
                dst_ref=rows.at[tp, first:last, :],
                send_sem=d_send.at[g, dx - 1],
                recv_sem=d_recv.at[g, dx - 1],
                device_id=(ep, (tp + dx) % lanes),
                device_id_type=MESH,
            )
            copy.start()
            chunk = [low <= g * per_group < top for low, top in CHUNKS].index(True)
            spreads[chunk].append((g, dx, first, last, copy))

    lane_id = iota((height, plane * TILE), 1)
    dz, dy = hop(lane_id // TILE, ring_z)
    expert = ((z + dz) % ring_z) * (RING_Y // 2) + ((y + dy) % RING_Y) // 2
    slot_of = expert * CAP + lane_id % CAP
    same_part = (lane_id % TILE) // CAP == iota((height, plane * TILE), 0) // seqs
    combine = jnp.zeros((height, plane * TILE), F32)
    for target, weight in zip(tall, tall_w):
        combine = combine + jnp.where((target == slot_of) & same_part, weight, 0.0)

    gives = []
    for c, (low, top) in enumerate(CHUNKS):
        here = slice(low * TILE, top * TILE)
        high = (top - low) * CAP
        sort, unsort = shuffles[c]
        for g, dx, first, last, copy in spreads[c]:
            source = (tp + lanes - dx) % lanes
            landed(rows.at[source, first:last, :], d_send.at[g, dx - 1], d_recv.at[g, dx - 1]).wait_recv()
        wide = jnp.concatenate([rows[x, here, :] for x in range(lanes)], axis=1)
        ordered = jnp.dot(sort, wide, preferred_element_type=F32)
        arrived = jnp.concatenate(
            [ordered[q * high : (q + 1) * high, x * LANE : (x + 1) * LANE] for x in range(lanes) for q in range(PARTS)],
            axis=1,
        )
        ffn_in = rms_scale(arrived, ffn_gain[...]).astype(BF16)
        if c == 0:
            for load in loads:
                load.wait()
            for swap in swaps:
                swap.wait_recv()
        units = []
        for s in range(CORES):
            both = jnp.dot(ffn_in, wide_in[s], preferred_element_type=F32)
            units.append((jax.nn.silu(both[:, :hidden]) * both[:, hidden:]).astype(BF16))
        part = jnp.dot(jnp.concatenate(units, axis=1), wdown[...], preferred_element_type=F32).astype(BF16)
        tall_part = jnp.concatenate(
            [
                jnp.concatenate([part[:, (x * PARTS + q) * LANE : (x * PARTS + q + 1) * LANE] for x in range(lanes)], axis=1)
                for q in range(PARTS)
            ],
            axis=0,
        )
        split = jnp.dot(unsort, tall_part, preferred_element_type=F32).astype(BF16)
        for x in range(lanes):
            ysend[x, here, :] = split[:, x * LANE : (x + 1) * LANE]
        for first, last in PIECES[c]:
            piece = slice(first * TILE, last * TILE)
            copies = []
            for dx in range(1, lanes):
                to = (tp + dx) % lanes
                copy = pltpu.make_async_remote_copy(
                    src_ref=ysend.at[to, piece, :],
                    dst_ref=yrecv.at[dx - 1, piece, :],
                    send_sem=f_send.at[len(gives), dx - 1],
                    recv_sem=f_recv.at[len(gives), dx - 1],
                    device_id=(ep, to),
                    device_id_type=MESH,
                )
                copy.start()
                copies.append(copy)
            gives.append((first, last, copies))

    for first, last, copies in gives:
        piece = slice(first * TILE, last * TILE)
        own = ysend[tp, piece, :].astype(F32)
        for dx, copy in enumerate(copies):
            copy.wait_recv()
            own = own + yrecv[dx, piece, :].astype(F32)
        gathered[piece, :] = own.astype(BF16)
        for slot in range(last - 1, max(1, first) - 1, -1):
            pltpu.make_async_remote_copy(
                src_ref=gathered.at[slot * TILE : (slot + 1) * TILE, :],
                dst_ref=back.at[slot * TILE : (slot + 1) * TILE, :],
                send_sem=g_send,
                recv_sem=g_recv,
                device_id=(backward(slot), tp),
                device_id_type=MESH,
            ).start()
        if first == 0:
            back[0:TILE, :] = gathered[0:TILE, :]

    for copy in sums:
        copy.wait_send()
    for swap in swaps:
        swap.wait_send()
    landed(gathered.at[TILE : plane * TILE, :], c_send, g_recv).wait_send()
    for copies in spreads:
        for _, _, _, _, copy in copies:
            copy.wait_send()
    for _, _, copies in gives:
        for copy in copies:
            copy.wait_send()
    landed(gathered.at[TILE : plane * TILE, :], g_send, g_recv).wait_send()

    landed(back.at[TILE : plane * TILE, :], g_send, g_recv).wait_recv()
    moe = jnp.dot(combine, back[...].astype(F32), preferred_element_type=F32, precision=HIGHEST)
    moe = jnp.concatenate([moe[q * seqs : (q + 1) * seqs] for q in range(PARTS)], axis=1)
    out_ref[...] = (resid.astype(F32) + moe).astype(BF16)


def exchange(
    readout, tokens, attn_gain, head_gain, ffn_gain, routes, route_weight, outgate_weight, output_weight, expert_gate,
    expert_up, expert_down,
):
    lanes, groups = lax.axis_size("tp"), lax.axis_size("ep")
    seqs, model = tokens.shape
    width = model // lanes
    plane = groups // CORES
    hidden = expert_gate.shape[2]
    anywhere = pl.BlockSpec(memory_space=pltpu.HBM)
    dma = pltpu.SemaphoreType.DMA
    small = (
        tokens, attn_gain.reshape(1, -1), head_gain.reshape(1, -1), ffn_gain.reshape(1, -1), routes.T, route_weight.T
    )
    weights = (outgate_weight, output_weight)
    vmem = pl.BlockSpec(memory_space=pltpu.VMEM)
    return pl.pallas_call(
        functools.partial(exchange_kernel, lanes, groups),
        name="exchange",
        out_shape=jax.ShapeDtypeStruct((seqs, width), BF16),
        in_specs=[vmem] * len(small) + [anywhere] * 6,
        out_specs=vmem,
        scratch_shapes=[pltpu.VMEM((seqs, readout.shape[1]), F32)]
        + [pltpu.VMEM(array.shape, array.dtype) for array in weights]
        + [
            pltpu.VMEM((seqs, model), BF16),
            pltpu.VMEM((lanes - 1, seqs, width), BF16),
            pltpu.VMEM((groups // 4 * TILE, LANE), BF16),
            pltpu.VMEM((lanes, plane * TILE, LANE), BF16),
            pltpu.VMEM((CORES, model, 2 * hidden), BF16),
            pltpu.VMEM((CORES * hidden, model), BF16),
            pltpu.VMEM((lanes, plane * TILE, LANE), BF16),
            pltpu.VMEM((lanes - 1, plane * TILE, LANE), BF16),
            pltpu.VMEM((plane * TILE, LANE), BF16),
            pltpu.VMEM((plane * TILE, LANE), BF16),
            pltpu.SemaphoreType.REGULAR,
            dma((3,)),
            dma((3,)),
            dma((3,)),
            dma((3,)),
            dma((lanes - 1,)),
            dma((lanes - 1,)),
            dma,
            dma((GROUPS,)),
            dma((GROUPS, lanes - 1)),
            dma((GROUPS, lanes - 1)),
            dma((sum(map(len, PIECES)), lanes - 1)),
            dma((sum(map(len, PIECES)), lanes - 1)),
            dma,
            dma,
        ],
        compiler_params=pltpu.CompilerParams(collective_id=0, has_side_effects=True, vmem_limit_bytes=EXCHANGE_GRANT),
    )(*small, readout, *weights, expert_gate, expert_up, expert_down)


def local(
    tokens,
    recur_state,
    attn_gain,
    query_weight,
    key_weight,
    value_weight,
    outgate_weight,
    beta_weight,
    decay_weight,
    decay_rate,
    head_gain,
    output_weight,
    ffn_gain,
    routes,
    route_weight,
    expert_gate,
    expert_up,
    expert_down,
):
    readout, new_state = mixer(
        tokens, recur_state, attn_gain, query_weight, key_weight, value_weight, beta_weight, decay_weight, decay_rate
    )
    mixed = exchange(
        readout, tokens, attn_gain, head_gain, ffn_gain, routes, route_weight, outgate_weight, output_weight, expert_gate,
        expert_up, expert_down,
    )
    return (mixed, new_state)


def solution(mesh):
    return jax.shard_map(
        local,
        mesh=mesh,
        in_specs=(
            P("ep", None),
            P("ep", "tp", None, None),
            P(),
            P(None, "tp"),
            P(None, "tp"),
            P(None, "tp"),
            P(None, "tp"),
            P(),
            P(),
            P(),
            P(),
            P("tp", None),
            P(),
            P("ep", None),
            P("ep", None),
            P("ep", None, "tp"),
            P("ep", None, "tp"),
            P("ep", "tp", None),
        ),
        out_specs=(P("ep", "tp"), P("ep", "tp", None, None)),
        check_vma=False,
    )
```

```python
import functools

import jax
import jax.numpy as jnp
from jax import lax
from jax.experimental import pallas as pl
from jax.experimental.pallas import tpu as pltpu
from jax.sharding import PartitionSpec as P

EPS = 1e-06
MESH = pl.DeviceIdType.MESH
F32 = jnp.float32
BF16 = jnp.bfloat16
HIGHEST = lax.Precision.HIGHEST
CORES = 2
RING_Y = 4
CAP = 4
PARTS = 4
LANE = 128
TILE = CAP * PARTS
GROUPS = 8
CHUNKS = ((0, 16), (16, 32))
PIECES = (((0, 16),), ((24, 32), (16, 24)))
STATE_CHUNKS = 4
VMEM_GRANT = 63 * 1024 * 1024
EXCHANGE_GRANT = 53 * 1024 * 1024


def rms_scale(values, gain):
    return values * lax.rsqrt(jnp.mean(values * values, axis=-1, keepdims=True) + EPS) * gain


def unit_rows(values):
    return values * lax.rsqrt(jnp.sum(values * values, axis=-1, keepdims=True) + EPS)


def hop(slot, ring_z):
    i, dy = slot // RING_Y, slot % RING_Y
    dz = (i % 2) * ((i + 1) // 2) + (1 - i % 2) * ((ring_z - i // 2) % ring_z)
    return dz, dy


def iota(shape, dim):
    return lax.broadcasted_iota(jnp.int32, shape, dim)


def fetch(pairs, sems):
    copies = [pltpu.make_async_copy(src, dst, sems.at[i]) for i, (src, dst) in enumerate(pairs)]
    for copy in copies:
        copy.start()
    return copies


def heads_of(proj):
    proj = proj.astype(BF16).astype(F32)
    return [jax.nn.silu(proj[:, at : at + LANE]) for at in range(0, proj.shape[1], LANE)]


def mixer_kernel(
    heads, tokens_hbm, gain_hbm, beta_hbm, decay_hbm, rate_hbm, k_hbm, q_hbm, v_hbm, state_hbm,
    read_hbm, new_hbm, tokens, gain, beta, decay, rate, wk, wq, wv, state, read, small_sem, load_sem, state_sem, out_sem,
    read_sem,
):
    tp = lax.axis_index("tp")
    seqs = tokens.shape[0]
    step = seqs // STATE_CHUNKS

    small = fetch(
        ((tokens_hbm, tokens), (gain_hbm, gain), (beta_hbm, beta), (decay_hbm, decay), (rate_hbm, rate)), small_sem
    )
    loads = fetch(((k_hbm, wk), (q_hbm, wq), (v_hbm, wv)), load_sem)
    parts = [pl.ds(c * step, step) for c in range(STATE_CHUNKS)]

    for copy in small + loads:
        copy.wait()
    reads = fetch([(state_hbm.at[part], state.at[part]) for part in parts], state_sem)
    normed = rms_scale(tokens[...].astype(F32), gain[...]).astype(BF16)

    def project(weight):
        return heads_of(jnp.dot(normed, weight[...], preferred_element_type=F32))

    keys = [unit_rows(k) for k in project(wk)]
    queries = [unit_rows(q) * LANE ** (-0.5) for q in project(wq)]
    values = project(wv)
    filler = [jnp.zeros((LANE - 2 * heads * seqs, LANE), F32)]
    columns = jnp.concatenate(keys + queries + filler, axis=0).T

    def by_head(weight):
        return lax.dot_general(normed, weight[...], (((1,), (1,)), ((), ())), preferred_element_type=F32)

    strength = jax.nn.sigmoid(by_head(beta))
    fading = jnp.exp(-rate[...] * jax.nn.softplus(by_head(decay)))

    def own_head(values, h):
        chosen = iota(values.shape, 1) == tp * heads + h
        column = jnp.sum(jnp.where(chosen, values, 0.0), axis=1, keepdims=True)
        return jnp.broadcast_to(column, (seqs, LANE))

    strengths = [own_head(strength, h) for h in range(heads)]
    fadings = [own_head(fading, h) for h in range(heads)]

    writes = []
    for c, part in enumerate(parts):
        reads[c].wait()
        for t in range(c * step, (c + 1) * step):
            for h in range(heads):
                j = h * seqs + t
                key, query = columns[:, j : j + 1], columns[:, heads * seqs + j : heads * seqs + j + 1]
                fade = fadings[h][t : t + 1]
                old = state[t, h]
                recall = jnp.sum(old * key, axis=0, keepdims=True)
                delta = strengths[h][t : t + 1] * (values[h][t : t + 1] - fade * recall)
                new = fade * old + key * delta
                state[t, h] = new
                read[t : t + 1, h * LANE : (h + 1) * LANE] = jnp.sum(new * query, axis=0, keepdims=True)
        write = pltpu.make_async_copy(state.at[part], new_hbm.at[part], out_sem.at[c])
        write.start()
        writes.append(write)
    write = pltpu.make_async_copy(read, read_hbm.at[0:seqs], read_sem)
    write.start()
    write.wait()
    for write in writes:
        write.wait()


def mixer(
    tokens, recur_state, attn_gain, query_weight, key_weight, value_weight, beta_weight, decay_weight, decay_rate
):
    seqs, model = tokens.shape
    heads, size = recur_state.shape[1:3]
    anywhere = pl.BlockSpec(memory_space=pltpu.HBM)
    dma = pltpu.SemaphoreType.DMA
    small = (tokens, attn_gain.reshape(1, -1), beta_weight.T, decay_weight.T, decay_rate.reshape(1, -1))
    return pl.pallas_call(
        functools.partial(mixer_kernel, heads),
        name="mixer",
        out_shape=(
            jax.ShapeDtypeStruct((model, heads * size), F32),
            jax.ShapeDtypeStruct(recur_state.shape, F32),
        ),
        in_specs=[anywhere] * 9,
        out_specs=(anywhere, anywhere),
        scratch_shapes=[pltpu.VMEM(array.shape, array.dtype) for array in small]
        + [pltpu.VMEM((model, heads * size), BF16)] * 3
        + [
            pltpu.VMEM(recur_state.shape, F32),
            pltpu.VMEM((seqs, heads * size), F32),
            dma((5,)),
            dma((3,)),
            dma((STATE_CHUNKS,)),
            dma((STATE_CHUNKS,)),
            dma,
        ],
        compiler_params=pltpu.CompilerParams(vmem_limit_bytes=VMEM_GRANT),
    )(*small, key_weight, query_weight, value_weight, recur_state)


def exchange_kernel(
    lanes, groups, tokens, attn_gain, head_gain, ffn_gain, routes_flat, rw_flat,
    read_hbm, z_hbm, o_hbm, gate_hbm, up_hbm, down_hbm, out_ref,
    read, wz, wo,
    partial, branch, packed, rows, wide_in, wdown, ysend, yrecv, gathered, back,
    ready, head_sem, local_sem, swap_send, swap_recv, b_send, b_recv, c_send, c_recv, d_send, d_recv,
    f_send, f_recv, g_send, g_recv,
):
    ring_z = groups // (RING_Y * CORES)
    plane = ring_z * RING_Y
    per_group = plane // GROUPS
    tp = lax.axis_index("tp")
    ep = lax.axis_index("ep")
    core = ep % CORES
    y = (ep // CORES) % RING_Y
    z = ep // (CORES * RING_Y)
    seqs, width = tokens.shape[0], tokens.shape[1] // lanes

    zs = [(z + dz) % ring_z for dz in range(ring_z)]
    ys = [(y + dy) % RING_Y for dy in range(RING_Y)]
    z_part = [zz * (RING_Y * CORES) for zz in zs]
    y_part = [yy * CORES + core for yy in ys]

    def forward(slot):
        dz, dy = hop(slot, ring_z)
        return z_part[dz] + y_part[dy]

    def backward(slot):
        dz, dy = hop(slot, ring_z)
        return z_part[-dz % ring_z] + y_part[-dy % RING_Y]

    partner = ep + 1 - 2 * core
    far_first = sorted(range(1, lanes), key=lambda dx: -min(dx, lanes - dx))
    nearest_last = list(range(plane - 1, 0, -1))

    z_in, read_in, o_in = fetch(((z_hbm, wz), (read_hbm.at[0:seqs], read), (o_hbm, wo)), head_sem)

    barrier = pltpu.get_barrier_semaphore()
    for slot in nearest_last:
        pl.semaphore_signal(barrier, inc=1, device_id=(forward(slot), tp), device_id_type=MESH)
    for dx in range(1, lanes):
        pl.semaphore_signal(barrier, inc=1, device_id=(ep, (tp + dx) % lanes), device_id_type=MESH)

    @pl.when(core == 0)
    def _():
        pl.semaphore_signal(barrier, inc=1, device_id=(partner, tp), device_id_type=MESH)

    hidden = gate_hbm.shape[2]

    def weights(s):
        return (
            (gate_hbm.at[0], wide_in.at[s, :, 0:hidden]),
            (up_hbm.at[0], wide_in.at[s, :, hidden : 2 * hidden]),
            (down_hbm.at[0], wdown.at[s * hidden : (s + 1) * hidden, :]),
        )

    loads = fetch(weights(0), local_sem)

    normed = rms_scale(tokens[...].astype(F32), attn_gain[...]).astype(BF16)
    z_in.wait()
    read_in.wait()
    gates = heads_of(jnp.dot(normed, wz[...], preferred_element_type=F32))
    headed = [
        (rms_scale(read[:, h * LANE : (h + 1) * LANE], head_gain[...]) * gate).astype(BF16) for h, gate in enumerate(gates)
    ]
    o_in.wait()
    shares = jnp.dot(jnp.concatenate(headed, axis=1), wo[...], preferred_element_type=F32)
    partial[...] = shares.astype(BF16)

    pl.semaphore_wait(barrier, plane - 1 + lanes - 1 + core)

    sums = []
    for dx in far_first:
        to = (tp + dx) % lanes
        copy = pltpu.make_async_remote_copy(
            src_ref=partial.at[:, pl.ds(pl.multiple_of(to * width, LANE), width)],
            dst_ref=branch.at[dx - 1],
            send_sem=b_send.at[dx - 1],
            recv_sem=b_recv.at[dx - 1],
            device_id=(ep, to),
            device_id_type=MESH,
        )
        copy.start()
        sums.append((dx, copy))

    swaps = [
        pltpu.make_async_remote_copy(
            src_ref=src, dst_ref=dst, send_sem=swap_send.at[i], recv_sem=swap_recv.at[i],
            device_id=(partner, tp), device_id_type=MESH,
        )
        for i, (src, dst) in enumerate(weights(1))
    ]

    @pl.when(core == 1)
    def _():
        pl.semaphore_signal(ready, inc=1, device_id=(partner, tp), device_id_type=MESH)
        for swap in swaps:
            swap.start()

    experts = groups // 4
    eye = (iota((seqs, seqs), 0) == iota((seqs, seqs), 1)).astype(F32)

    def upright(flat):
        return lax.dot_general(eye, flat, (((1,), (1,)), ((), ())), preferred_element_type=F32, precision=HIGHEST)

    routes = upright(routes_flat[...].astype(F32)).astype(jnp.int32)
    rw = upright(rw_flat[...])
    onehots = [(routes[:, k : k + 1] == iota((seqs, experts), 1)).astype(F32) for k in range(routes.shape[1])]
    earlier = (iota((seqs, seqs), 1) < iota((seqs, seqs), 0)).astype(F32)
    counts = jnp.dot(earlier, sum(onehots), preferred_element_type=F32)
    targets = []
    for k, onehot in enumerate(onehots):
        position = jnp.sum(counts * onehot, axis=1, keepdims=True).astype(jnp.int32)
        targets.append(routes[:, k : k + 1] * CAP + position)
    tall = [jnp.concatenate([t] * PARTS, axis=0) for t in targets]
    tall_w = [jnp.concatenate([rw[:, k : k + 1]] * PARTS, axis=0) for k in range(len(targets))]
    height = PARTS * seqs
    lane_id = iota((height, experts * TILE), 1)
    slot_of = (lane_id // TILE) * CAP + lane_id % CAP
    same_part = (lane_id % TILE) // CAP == iota((height, experts * TILE), 0) // seqs
    chosen = (tall[0] == slot_of) | (tall[1] == slot_of)
    select = (chosen & same_part).astype(F32).astype(BF16)

    mine = pl.ds(pl.multiple_of(tp * width, LANE), width)
    total = partial[:, mine].astype(F32)
    for dx, copy in sums:
        copy.wait_recv()
        total = total + branch[dx - 1].astype(F32)
    resid = (tokens[:, mine].astype(F32) + total.astype(BF16).astype(F32)).astype(BF16)
    stacked = jnp.concatenate([resid[:, q * LANE : (q + 1) * LANE] for q in range(PARTS)], axis=0)
    picked = lax.dot_general(select, stacked, (((0,), (0,)), ((), ())), preferred_element_type=F32)
    packed[...] = picked.astype(BF16)

    z_rows = [zz * (RING_Y // 2 * TILE) for zz in zs]
    y_rows = [yy // 2 * TILE for yy in ys]
    for slot in range(1, plane):
        dz, dy = hop(slot, ring_z)
        pltpu.make_async_remote_copy(
            src_ref=packed.at[pl.ds(pl.multiple_of(z_rows[dz] + y_rows[dy], TILE), TILE), :],
            dst_ref=rows.at[tp, slot * TILE : (slot + 1) * TILE, :],
            send_sem=c_send,
            recv_sem=c_recv.at[slot // per_group],
            device_id=(forward(slot), tp),
            device_id_type=MESH,
        ).start()

    rows[tp, 0:TILE, :] = packed[pl.ds(pl.multiple_of(z_rows[0] + y_rows[0], TILE), TILE), :]

    @pl.when(core == 0)
    def _():
        pl.semaphore_wait(ready, 1)
        for swap in swaps:
            swap.start()

    def landed(ref, send_sem, recv_sem):
        return pltpu.make_async_remote_copy(
            src_ref=ref, dst_ref=ref, send_sem=send_sem, recv_sem=recv_sem, device_id=(partner, tp), device_id_type=MESH
        )

    def shuffle(slots):
        high = slots * CAP
        shape = (slots * TILE, slots * TILE)

        def hit(dim):
            index = iota(shape, dim)
            part = sum((index >= q * high).astype(jnp.int32) for q in range(1, PARTS))
            rest = index - part * high
            return ((rest // CAP) * TILE + part * CAP + rest % CAP == iota(shape, 1 - dim)).astype(F32).astype(BF16)

        return hit(0), hit(1)

    shuffles = [shuffle(last - first) for first, last in CHUNKS]

    spreads = [[] for _ in CHUNKS]
    for g in range(GROUPS):
        first, last = g * per_group * TILE, (g + 1) * per_group * TILE
        fresh = max(first, TILE)
        landed(rows.at[tp, fresh:last, :], c_send, c_recv.at[g]).wait_recv()
        for dx in far_first:
            copy = pltpu.make_async_remote_copy(
                src_ref=rows.at[tp, first:last, :],
                dst_ref=rows.at[tp, first:last, :],
                send_sem=d_send.at[g, dx - 1],
                recv_sem=d_recv.at[g, dx - 1],
                device_id=(ep, (tp + dx) % lanes),
                device_id_type=MESH,
            )
            copy.start()
            chunk = [low <= g * per_group < top for low, top in CHUNKS].index(True)
            spreads[chunk].append((g, dx, first, last, copy))

    lane_id = iota((height, plane * TILE), 1)
    dz, dy = hop(lane_id // TILE, ring_z)
    expert = ((z + dz) % ring_z) * (RING_Y // 2) + ((y + dy) % RING_Y) // 2
    slot_of = expert * CAP + lane_id % CAP
    same_part = (lane_id % TILE) // CAP == iota((height, plane * TILE), 0) // seqs
    combine = jnp.zeros((height, plane * TILE), F32)
    for target, weight in zip(tall, tall_w):
        combine = combine + jnp.where((target == slot_of) & same_part, weight, 0.0)
    thirds = []
    for _ in range(3):
        thirds.append(combine.astype(BF16))
        combine = combine - thirds[-1].astype(F32)
    combine = jnp.concatenate(thirds, axis=0)

    gives = []
    for c, (low, top) in enumerate(CHUNKS):
        here = slice(low * TILE, top * TILE)
        high = (top - low) * CAP
        sort, unsort = shuffles[c]
        for g, dx, first, last, copy in spreads[c]:
            source = (tp + lanes - dx) % lanes
            landed(rows.at[source, first:last, :], d_send.at[g, dx - 1], d_recv.at[g, dx - 1]).wait_recv()
        wide = jnp.concatenate([rows[x, here, :] for x in range(lanes)], axis=1)
        ordered = jnp.dot(sort, wide, preferred_element_type=F32)
        arrived = jnp.concatenate(
            [ordered[q * high : (q + 1) * high, x * LANE : (x + 1) * LANE] for x in range(lanes) for q in range(PARTS)],
            axis=1,
        )
        ffn_in = rms_scale(arrived, ffn_gain[...]).astype(BF16)
        if c == 0:
            for load in loads:
                load.wait()
            for swap in swaps:
                swap.wait_recv()
        units = []
        for s in range(CORES):
            both = jnp.dot(ffn_in, wide_in[s], preferred_element_type=F32)
            units.append((jax.nn.silu(both[:, :hidden]) * both[:, hidden:]).astype(BF16))
        part = jnp.dot(jnp.concatenate(units, axis=1), wdown[...], preferred_element_type=F32).astype(BF16)
        tall_part = jnp.concatenate(
            [
                jnp.concatenate([part[:, (x * PARTS + q) * LANE : (x * PARTS + q + 1) * LANE] for x in range(lanes)], axis=1)
                for q in range(PARTS)
            ],
            axis=0,
        )
        split = jnp.dot(unsort, tall_part, preferred_element_type=F32).astype(BF16)
        for x in range(lanes):
            ysend[x, here, :] = split[:, x * LANE : (x + 1) * LANE]
        for first, last in PIECES[c]:
            piece = slice(first * TILE, last * TILE)
            copies = []
            for dx in far_first:
                to = (tp + dx) % lanes
                copy = pltpu.make_async_remote_copy(
                    src_ref=ysend.at[to, piece, :],
                    dst_ref=yrecv.at[dx - 1, piece, :],
                    send_sem=f_send.at[len(gives), dx - 1],
                    recv_sem=f_recv.at[len(gives), dx - 1],
                    device_id=(ep, to),
                    device_id_type=MESH,
                )
                copy.start()
                copies.append((dx, copy))
            gives.append((first, last, copies))

    for first, last, copies in gives:
        piece = slice(first * TILE, last * TILE)
        own = ysend[tp, piece, :].astype(F32)
        for dx, copy in sorted(copies, key=lambda pair: pair[0]):
            copy.wait_recv()
            own = own + yrecv[dx - 1, piece, :].astype(F32)
        gathered[piece, :] = own.astype(BF16)
        for slot in range(last - 1, max(1, first) - 1, -1):
            pltpu.make_async_remote_copy(
                src_ref=gathered.at[slot * TILE : (slot + 1) * TILE, :],
                dst_ref=back.at[slot * TILE : (slot + 1) * TILE, :],
                send_sem=g_send,
                recv_sem=g_recv,
                device_id=(backward(slot), tp),
                device_id_type=MESH,
            ).start()
        if first == 0:
            back[0:TILE, :] = gathered[0:TILE, :]

    for _, copy in sums:
        copy.wait_send()
    for swap in swaps:
        swap.wait_send()
    landed(gathered.at[TILE : plane * TILE, :], c_send, g_recv).wait_send()
    for copies in spreads:
        for _, _, _, _, copy in copies:
            copy.wait_send()
    for _, _, copies in gives:
        for _, copy in copies:
            copy.wait_send()
    landed(gathered.at[TILE : plane * TILE, :], g_send, g_recv).wait_send()

    landed(back.at[TILE : plane * TILE, :], g_send, g_recv).wait_recv()
    thirds = jnp.dot(combine, back[...], preferred_element_type=F32)
    moe = thirds[:height] + thirds[height : 2 * height] + thirds[2 * height :]
    moe = jnp.concatenate([moe[q * seqs : (q + 1) * seqs] for q in range(PARTS)], axis=1)
    out_ref[...] = (resid.astype(F32) + moe).astype(BF16)


def exchange(
    readout, tokens, attn_gain, head_gain, ffn_gain, routes, route_weight, outgate_weight, output_weight, expert_gate,
    expert_up, expert_down,
):
    lanes, groups = lax.axis_size("tp"), lax.axis_size("ep")
    seqs, model = tokens.shape
    width = model // lanes
    plane = groups // CORES
    hidden = expert_gate.shape[2]
    anywhere = pl.BlockSpec(memory_space=pltpu.HBM)
    dma = pltpu.SemaphoreType.DMA
    small = (
        tokens, attn_gain.reshape(1, -1), head_gain.reshape(1, -1), ffn_gain.reshape(1, -1), routes.T, route_weight.T
    )
    weights = (outgate_weight, output_weight)
    vmem = pl.BlockSpec(memory_space=pltpu.VMEM)
    return pl.pallas_call(
        functools.partial(exchange_kernel, lanes, groups),
        name="exchange",
        out_shape=jax.ShapeDtypeStruct((seqs, width), BF16),
        in_specs=[vmem] * len(small) + [anywhere] * 6,
        out_specs=vmem,
        scratch_shapes=[pltpu.VMEM((seqs, readout.shape[1]), F32)]
        + [pltpu.VMEM(array.shape, array.dtype) for array in weights]
        + [
            pltpu.VMEM((seqs, model), BF16),
            pltpu.VMEM((lanes - 1, seqs, width), BF16),
            pltpu.VMEM((groups // 4 * TILE, LANE), BF16),
            pltpu.VMEM((lanes, plane * TILE, LANE), BF16),
            pltpu.VMEM((CORES, model, 2 * hidden), BF16),
            pltpu.VMEM((CORES * hidden, model), BF16),
            pltpu.VMEM((lanes, plane * TILE, LANE), BF16),
            pltpu.VMEM((lanes - 1, plane * TILE, LANE), BF16),
            pltpu.VMEM((plane * TILE, LANE), BF16),
            pltpu.VMEM((plane * TILE, LANE), BF16),
            pltpu.SemaphoreType.REGULAR,
            dma((3,)),
            dma((3,)),
            dma((3,)),
            dma((3,)),
            dma((lanes - 1,)),
            dma((lanes - 1,)),
            dma,
            dma((GROUPS,)),
            dma((GROUPS, lanes - 1)),
            dma((GROUPS, lanes - 1)),
            dma((sum(map(len, PIECES)), lanes - 1)),
            dma((sum(map(len, PIECES)), lanes - 1)),
            dma,
            dma,
        ],
        compiler_params=pltpu.CompilerParams(collective_id=0, has_side_effects=True, vmem_limit_bytes=EXCHANGE_GRANT),
    )(*small, readout, *weights, expert_gate, expert_up, expert_down)


def local(
    tokens,
    recur_state,
    attn_gain,
    query_weight,
    key_weight,
    value_weight,
    outgate_weight,
    beta_weight,
    decay_weight,
    decay_rate,
    head_gain,
    output_weight,
    ffn_gain,
    routes,
    route_weight,
    expert_gate,
    expert_up,
    expert_down,
):
    readout, new_state = mixer(
        tokens, recur_state, attn_gain, query_weight, key_weight, value_weight, beta_weight, decay_weight, decay_rate
    )
    mixed = exchange(
        readout, tokens, attn_gain, head_gain, ffn_gain, routes, route_weight, outgate_weight, output_weight, expert_gate,
        expert_up, expert_down,
    )
    return (mixed, new_state)


def solution(mesh):
    return jax.shard_map(
        local,
        mesh=mesh,
        in_specs=(
            P("ep", None),
            P("ep", "tp", None, None),
            P(),
            P(None, "tp"),
            P(None, "tp"),
            P(None, "tp"),
            P(None, "tp"),
            P(),
            P(),
            P(),
            P(),
            P("tp", None),
            P(),
            P("ep", None),
            P("ep", None),
            P("ep", None, "tp"),
            P("ep", None, "tp"),
            P("ep", "tp", None),
        ),
        out_specs=(P("ep", "tp"), P("ep", "tp", None, None)),
        check_vma=False,
    )
```

```python
import functools

import jax
import jax.numpy as jnp
from jax import lax
from jax.experimental import pallas as pl
from jax.experimental.pallas import tpu as pltpu
from jax.sharding import PartitionSpec as P

EPS = 1e-06
MESH = pl.DeviceIdType.MESH
F32 = jnp.float32
BF16 = jnp.bfloat16
HIGHEST = lax.Precision.HIGHEST
CORES = 2
RING_Y = 4
CAP = 4
PARTS = 4
LANE = 128
TILE = CAP * PARTS
GROUPS = 8
CHUNKS = ((0, 16), (16, 32))
PIECES = (((0, 16),), ((24, 32), (16, 24)))
STATE_CHUNKS = 4
VMEM_GRANT = 63 * 1024 * 1024
EXCHANGE_GRANT = 53 * 1024 * 1024


def rms_scale(values, gain):
    return values * lax.rsqrt(jnp.mean(values * values, axis=-1, keepdims=True) + EPS) * gain


def unit_rows(values):
    return values * lax.rsqrt(jnp.sum(values * values, axis=-1, keepdims=True) + EPS)


def hop(slot, ring_z):
    i, dy = slot // RING_Y, slot % RING_Y
    dz = (i % 2) * ((i + 1) // 2) + (1 - i % 2) * ((ring_z - i // 2) % ring_z)
    return dz, dy


def iota(shape, dim):
    return lax.broadcasted_iota(jnp.int32, shape, dim)


def fetch(pairs, sems):
    copies = [pltpu.make_async_copy(src, dst, sems.at[i]) for i, (src, dst) in enumerate(pairs)]
    for copy in copies:
        copy.start()
    return copies


def heads_of(proj):
    proj = proj.astype(BF16).astype(F32)
    return [jax.nn.silu(proj[:, at : at + LANE]) for at in range(0, proj.shape[1], LANE)]


def mixer_kernel(
    heads, tokens_hbm, gain_hbm, beta_hbm, decay_hbm, rate_hbm, k_hbm, q_hbm, v_hbm, state_hbm,
    read_hbm, new_hbm, tokens, gain, beta, decay, rate, wk, wq, wv, state, read, small_sem, load_sem, state_sem, out_sem,
    read_sem,
):
    tp = lax.axis_index("tp")
    seqs = tokens.shape[0]
    step = seqs // STATE_CHUNKS

    small = fetch(
        ((tokens_hbm, tokens), (gain_hbm, gain), (beta_hbm, beta), (decay_hbm, decay), (rate_hbm, rate)), small_sem
    )
    loads = fetch(((k_hbm, wk), (q_hbm, wq), (v_hbm, wv)), load_sem)
    parts = [pl.ds(c * step, step) for c in range(STATE_CHUNKS)]

    for copy in small + loads:
        copy.wait()
    reads = fetch([(state_hbm.at[part], state.at[part]) for part in parts], state_sem)
    normed = rms_scale(tokens[...].astype(F32), gain[...]).astype(BF16)

    def project(weight):
        return heads_of(jnp.dot(normed, weight[...], preferred_element_type=F32))

    keys = [unit_rows(k) for k in project(wk)]
    queries = [unit_rows(q) * LANE ** (-0.5) for q in project(wq)]
    values = project(wv)
    filler = [jnp.zeros((LANE - 2 * heads * seqs, LANE), F32)]
    columns = jnp.concatenate(keys + queries + filler, axis=0).T

    def by_head(weight):
        return lax.dot_general(normed, weight[...], (((1,), (1,)), ((), ())), preferred_element_type=F32)

    strength = jax.nn.sigmoid(by_head(beta))
    fading = jnp.exp(-rate[...] * jax.nn.softplus(by_head(decay)))

    def own_head(values, h):
        chosen = iota(values.shape, 1) == tp * heads + h
        column = jnp.sum(jnp.where(chosen, values, 0.0), axis=1, keepdims=True)
        return jnp.broadcast_to(column, (seqs, LANE))

    strengths = [own_head(strength, h) for h in range(heads)]
    fadings = [own_head(fading, h) for h in range(heads)]

    writes = []
    for c, part in enumerate(parts):
        reads[c].wait()
        for t in range(c * step, (c + 1) * step):
            for h in range(heads):
                j = h * seqs + t
                key, query = columns[:, j : j + 1], columns[:, heads * seqs + j : heads * seqs + j + 1]
                fade = fadings[h][t : t + 1]
                old = state[t, h]
                recall = jnp.sum(old * key, axis=0, keepdims=True)
                delta = strengths[h][t : t + 1] * (values[h][t : t + 1] - fade * recall)
                new = fade * old + key * delta
                state[t, h] = new
                read[t : t + 1, h * LANE : (h + 1) * LANE] = jnp.sum(new * query, axis=0, keepdims=True)
        write = pltpu.make_async_copy(state.at[part], new_hbm.at[part], out_sem.at[c])
        write.start()
        writes.append(write)
    write = pltpu.make_async_copy(read, read_hbm.at[0:seqs], read_sem)
    write.start()
    write.wait()
    for write in writes:
        write.wait()


def mixer(
    tokens, recur_state, attn_gain, query_weight, key_weight, value_weight, beta_weight, decay_weight, decay_rate
):
    seqs, model = tokens.shape
    heads, size = recur_state.shape[1:3]
    anywhere = pl.BlockSpec(memory_space=pltpu.HBM)
    dma = pltpu.SemaphoreType.DMA
    small = (tokens, attn_gain.reshape(1, -1), beta_weight.T, decay_weight.T, decay_rate.reshape(1, -1))
    return pl.pallas_call(
        functools.partial(mixer_kernel, heads),
        name="mixer",
        out_shape=(
            jax.ShapeDtypeStruct((model, heads * size), F32),
            jax.ShapeDtypeStruct(recur_state.shape, F32),
        ),
        in_specs=[anywhere] * 9,
        out_specs=(anywhere, anywhere),
        scratch_shapes=[pltpu.VMEM(array.shape, array.dtype) for array in small]
        + [pltpu.VMEM((model, heads * size), BF16)] * 3
        + [
            pltpu.VMEM(recur_state.shape, F32),
            pltpu.VMEM((seqs, heads * size), F32),
            dma((5,)),
            dma((3,)),
            dma((STATE_CHUNKS,)),
            dma((STATE_CHUNKS,)),
            dma,
        ],
        compiler_params=pltpu.CompilerParams(vmem_limit_bytes=VMEM_GRANT),
    )(*small, key_weight, query_weight, value_weight, recur_state)


def exchange_kernel(
    lanes, groups, tokens, attn_gain, head_gain, ffn_gain, routes_flat, rw_flat,
    read_hbm, z_hbm, o_hbm, gate_hbm, up_hbm, down_hbm, out_ref,
    read, wz, wo,
    partial, branch, packed, rows, wide_in, wdown, ysend, yrecv, gathered, back,
    ready, head_sem, local_sem, swap_send, swap_recv, b_send, b_recv, c_send, c_recv, d_send, d_recv,
    f_send, f_recv, g_send, g_recv,
):
    ring_z = groups // (RING_Y * CORES)
    plane = ring_z * RING_Y
    per_group = plane // GROUPS
    tp = lax.axis_index("tp")
    ep = lax.axis_index("ep")
    core = ep % CORES
    y = (ep // CORES) % RING_Y
    z = ep // (CORES * RING_Y)
    seqs, width = tokens.shape[0], tokens.shape[1] // lanes

    zs = [(z + dz) % ring_z for dz in range(ring_z)]
    ys = [(y + dy) % RING_Y for dy in range(RING_Y)]
    z_part = [zz * (RING_Y * CORES) for zz in zs]
    y_part = [yy * CORES + core for yy in ys]

    def forward(slot):
        dz, dy = hop(slot, ring_z)
        return z_part[dz] + y_part[dy]

    def backward(slot):
        dz, dy = hop(slot, ring_z)
        return z_part[-dz % ring_z] + y_part[-dy % RING_Y]

    partner = ep + 1 - 2 * core
    far_first = sorted(range(1, lanes), key=lambda dx: -min(dx, lanes - dx))
    nearest_last = list(range(plane - 1, 0, -1))

    z_in, read_in, o_in = fetch(((z_hbm, wz), (read_hbm.at[0:seqs], read), (o_hbm, wo)), head_sem)

    barrier = pltpu.get_barrier_semaphore()
    for slot in nearest_last:
        pl.semaphore_signal(barrier, inc=1, device_id=(forward(slot), tp), device_id_type=MESH)
    for dx in range(1, lanes):
        pl.semaphore_signal(barrier, inc=1, device_id=(ep, (tp + dx) % lanes), device_id_type=MESH)

    @pl.when(core == 0)
    def _():
        pl.semaphore_signal(barrier, inc=1, device_id=(partner, tp), device_id_type=MESH)

    hidden = gate_hbm.shape[2]

    def weights(s):
        return (
            (gate_hbm.at[0], wide_in.at[s, :, 0:hidden]),
            (up_hbm.at[0], wide_in.at[s, :, hidden : 2 * hidden]),
            (down_hbm.at[0], wdown.at[s * hidden : (s + 1) * hidden, :]),
        )

    loads = fetch(weights(0), local_sem)

    normed = rms_scale(tokens[...].astype(F32), attn_gain[...]).astype(BF16)
    z_in.wait()
    read_in.wait()
    gates = heads_of(jnp.dot(normed, wz[...], preferred_element_type=F32))
    headed = [
        (rms_scale(read[:, h * LANE : (h + 1) * LANE], head_gain[...]) * gate).astype(BF16) for h, gate in enumerate(gates)
    ]
    o_in.wait()
    shares = jnp.dot(jnp.concatenate(headed, axis=1), wo[...], preferred_element_type=F32)
    partial[...] = shares.astype(BF16)

    pl.semaphore_wait(barrier, plane - 1 + lanes - 1 + core)

    sums = []
    for dx in far_first:
        to = (tp + dx) % lanes
        copy = pltpu.make_async_remote_copy(
            src_ref=partial.at[:, pl.ds(pl.multiple_of(to * width, LANE), width)],
            dst_ref=branch.at[dx - 1],
            send_sem=b_send.at[dx - 1],
            recv_sem=b_recv.at[dx - 1],
            device_id=(ep, to),
            device_id_type=MESH,
        )
        copy.start()
        sums.append((dx, copy))

    swaps = [
        pltpu.make_async_remote_copy(
            src_ref=src, dst_ref=dst, send_sem=swap_send.at[i], recv_sem=swap_recv.at[i],
            device_id=(partner, tp), device_id_type=MESH,
        )
        for i, (src, dst) in enumerate(weights(1))
    ]

    @pl.when(core == 1)
    def _():
        pl.semaphore_signal(ready, inc=1, device_id=(partner, tp), device_id_type=MESH)
        for swap in swaps:
            swap.start()

    experts = groups // 4
    eye = (iota((seqs, seqs), 0) == iota((seqs, seqs), 1)).astype(F32)

    def upright(flat):
        return lax.dot_general(eye, flat, (((1,), (1,)), ((), ())), preferred_element_type=F32, precision=HIGHEST)

    routes = upright(routes_flat[...].astype(F32)).astype(jnp.int32)
    rw = upright(rw_flat[...])
    onehots = [(routes[:, k : k + 1] == iota((seqs, experts), 1)).astype(F32) for k in range(routes.shape[1])]
    earlier = (iota((seqs, seqs), 1) < iota((seqs, seqs), 0)).astype(F32)
    counts = jnp.dot(earlier, sum(onehots), preferred_element_type=F32)
    targets = []
    for k, onehot in enumerate(onehots):
        position = jnp.sum(counts * onehot, axis=1, keepdims=True).astype(jnp.int32)
        targets.append(routes[:, k : k + 1] * CAP + position)
    tall = [jnp.concatenate([t] * PARTS, axis=0) for t in targets]
    tall_w = [jnp.concatenate([rw[:, k : k + 1]] * PARTS, axis=0) for k in range(len(targets))]
    height = PARTS * seqs
    lane_id = iota((height, experts * TILE), 1)
    slot_of = (lane_id // TILE) * CAP + lane_id % CAP
    same_part = (lane_id % TILE) // CAP == iota((height, experts * TILE), 0) // seqs
    chosen = (tall[0] == slot_of) | (tall[1] == slot_of)
    select = (chosen & same_part).astype(F32).astype(BF16)

    mine = pl.ds(pl.multiple_of(tp * width, LANE), width)
    total = partial[:, mine].astype(F32)
    for dx, copy in sums:
        copy.wait_recv()
        total = total + branch[dx - 1].astype(F32)
    resid = (tokens[:, mine].astype(F32) + total.astype(BF16).astype(F32)).astype(BF16)
    stacked = jnp.concatenate([resid[:, q * LANE : (q + 1) * LANE] for q in range(PARTS)], axis=0)
    picked = lax.dot_general(select, stacked, (((0,), (0,)), ((), ())), preferred_element_type=F32)
    packed[...] = picked.astype(BF16)

    z_rows = [zz * (RING_Y // 2 * TILE) for zz in zs]
    y_rows = [yy // 2 * TILE for yy in ys]
    for slot in range(1, plane):
        dz, dy = hop(slot, ring_z)
        pltpu.make_async_remote_copy(
            src_ref=packed.at[pl.ds(pl.multiple_of(z_rows[dz] + y_rows[dy], TILE), TILE), :],
            dst_ref=rows.at[tp, slot * TILE : (slot + 1) * TILE, :],
            send_sem=c_send,
            recv_sem=c_recv.at[slot // per_group],
            device_id=(forward(slot), tp),
            device_id_type=MESH,
        ).start()

    rows[tp, 0:TILE, :] = packed[pl.ds(pl.multiple_of(z_rows[0] + y_rows[0], TILE), TILE), :]

    @pl.when(core == 0)
    def _():
        pl.semaphore_wait(ready, 1)
        for swap in swaps:
            swap.start()

    def landed(ref, send_sem, recv_sem):
        return pltpu.make_async_remote_copy(
            src_ref=ref, dst_ref=ref, send_sem=send_sem, recv_sem=recv_sem, device_id=(partner, tp), device_id_type=MESH
        )

    def shuffle(slots):
        high = slots * CAP
        shape = (slots * TILE, slots * TILE)

        def hit(dim):
            index = iota(shape, dim)
            part = sum((index >= q * high).astype(jnp.int32) for q in range(1, PARTS))
            rest = index - part * high
            return ((rest // CAP) * TILE + part * CAP + rest % CAP == iota(shape, 1 - dim)).astype(F32).astype(BF16)

        return hit(0), hit(1)

    shuffles = [shuffle(last - first) for first, last in CHUNKS]

    spreads = [[] for _ in CHUNKS]
    for g in range(GROUPS):
        first, last = g * per_group * TILE, (g + 1) * per_group * TILE
        fresh = max(first, TILE)
        landed(rows.at[tp, fresh:last, :], c_send, c_recv.at[g]).wait_recv()
        for dx in far_first:
            copy = pltpu.make_async_remote_copy(
                src_ref=rows.at[tp, first:last, :],
                dst_ref=rows.at[tp, first:last, :],
                send_sem=d_send.at[g, dx - 1],
                recv_sem=d_recv.at[g, dx - 1],
                device_id=(ep, (tp + dx) % lanes),
                device_id_type=MESH,
            )
            copy.start()
            chunk = [low <= g * per_group < top for low, top in CHUNKS].index(True)
            spreads[chunk].append((g, dx, first, last, copy))

    lane_id = iota((height, plane * TILE), 1)
    dz, dy = hop(lane_id // TILE, ring_z)
    expert = ((z + dz) % ring_z) * (RING_Y // 2) + ((y + dy) % RING_Y) // 2
    slot_of = expert * CAP + lane_id % CAP
    same_part = (lane_id % TILE) // CAP == iota((height, plane * TILE), 0) // seqs
    combine = jnp.zeros((height, plane * TILE), F32)
    for target, weight in zip(tall, tall_w):
        combine = combine + jnp.where((target == slot_of) & same_part, weight, 0.0)
    thirds = []
    for _ in range(3):
        thirds.append(combine.astype(BF16))
        combine = combine - thirds[-1].astype(F32)
    combine = jnp.concatenate(thirds, axis=0)

    gives = []
    for c, (low, top) in enumerate(CHUNKS):
        here = slice(low * TILE, top * TILE)
        high = (top - low) * CAP
        sort, unsort = shuffles[c]
        for g, dx, first, last, copy in spreads[c]:
            source = (tp + lanes - dx) % lanes
            landed(rows.at[source, first:last, :], d_send.at[g, dx - 1], d_recv.at[g, dx - 1]).wait_recv()
        wide = jnp.concatenate([rows[x, here, :] for x in range(lanes)], axis=1)
        ordered = jnp.dot(sort, wide, preferred_element_type=F32)
        arrived = jnp.concatenate(
            [ordered[q * high : (q + 1) * high, x * LANE : (x + 1) * LANE] for x in range(lanes) for q in range(PARTS)],
            axis=1,
        )
        ffn_in = rms_scale(arrived, ffn_gain[...]).astype(BF16)
        if c == 0:
            for load in loads:
                load.wait()
            for swap in swaps:
                swap.wait_recv()
        units = []
        for s in range(CORES):
            both = jnp.dot(ffn_in, wide_in[s], preferred_element_type=F32)
            units.append((jax.nn.silu(both[:, :hidden]) * both[:, hidden:]).astype(BF16))
        part = jnp.dot(jnp.concatenate(units, axis=1), wdown[...], preferred_element_type=F32).astype(BF16)
        tall_part = jnp.concatenate(
            [
                jnp.concatenate([part[:, (x * PARTS + q) * LANE : (x * PARTS + q + 1) * LANE] for x in range(lanes)], axis=1)
                for q in range(PARTS)
            ],
            axis=0,
        )
        split = jnp.dot(unsort, tall_part, preferred_element_type=F32).astype(BF16)
        for x in range(lanes):
            ysend[x, here, :] = split[:, x * LANE : (x + 1) * LANE]
        for first, last in PIECES[c]:
            piece = slice(first * TILE, last * TILE)
            copies = []
            for dx in far_first:
                to = (tp + dx) % lanes
                copy = pltpu.make_async_remote_copy(
                    src_ref=ysend.at[to, piece, :],
                    dst_ref=yrecv.at[dx - 1, piece, :],
                    send_sem=f_send.at[len(gives), dx - 1],
                    recv_sem=f_recv.at[len(gives), dx - 1],
                    device_id=(ep, to),
                    device_id_type=MESH,
                )
                copy.start()
                copies.append((dx, copy))
            gives.append((first, last, copies))

    for first, last, copies in gives:
        piece = slice(first * TILE, last * TILE)
        own = ysend[tp, piece, :].astype(F32)
        for dx, copy in sorted(copies, key=lambda pair: pair[0]):
            copy.wait_recv()
            own = own + yrecv[dx - 1, piece, :].astype(F32)
        gathered[piece, :] = own.astype(BF16)
        for slot in range(last - 1, max(1, first) - 1, -1):
            pltpu.make_async_remote_copy(
                src_ref=gathered.at[slot * TILE : (slot + 1) * TILE, :],
                dst_ref=back.at[slot * TILE : (slot + 1) * TILE, :],
                send_sem=g_send,
                recv_sem=g_recv.at[slot * 2 // plane],
                device_id=(backward(slot), tp),
                device_id_type=MESH,
            ).start()
        if first == 0:
            back[0:TILE, :] = gathered[0:TILE, :]

    for _, copy in sums:
        copy.wait_send()
    for swap in swaps:
        swap.wait_send()
    landed(gathered.at[TILE : plane * TILE, :], c_send, g_recv.at[0]).wait_send()
    for copies in spreads:
        for _, _, _, _, copy in copies:
            copy.wait_send()
    for _, _, copies in gives:
        for _, copy in copies:
            copy.wait_send()
    landed(gathered.at[TILE : plane * TILE, :], g_send, g_recv.at[0]).wait_send()

    middle = plane // 2 * TILE
    moe = jnp.zeros((height, LANE), F32)
    for half, (first, fresh, last) in enumerate(((0, TILE, middle), (middle, middle, plane * TILE))):
        landed(back.at[fresh:last, :], g_send, g_recv.at[half]).wait_recv()
        thirds = jnp.dot(combine[:, first:last], back[first:last, :], preferred_element_type=F32)
        moe = moe + (thirds[:height] + thirds[height : 2 * height] + thirds[2 * height :])
    moe = jnp.concatenate([moe[q * seqs : (q + 1) * seqs] for q in range(PARTS)], axis=1)
    out_ref[...] = (resid.astype(F32) + moe).astype(BF16)


def exchange(
    readout, tokens, attn_gain, head_gain, ffn_gain, routes, route_weight, outgate_weight, output_weight, expert_gate,
    expert_up, expert_down,
):
    lanes, groups = lax.axis_size("tp"), lax.axis_size("ep")
    seqs, model = tokens.shape
    width = model // lanes
    plane = groups // CORES
    hidden = expert_gate.shape[2]
    anywhere = pl.BlockSpec(memory_space=pltpu.HBM)
    dma = pltpu.SemaphoreType.DMA
    small = (
        tokens, attn_gain.reshape(1, -1), head_gain.reshape(1, -1), ffn_gain.reshape(1, -1), routes.T, route_weight.T
    )
    weights = (outgate_weight, output_weight)
    vmem = pl.BlockSpec(memory_space=pltpu.VMEM)
    return pl.pallas_call(
        functools.partial(exchange_kernel, lanes, groups),
        name="exchange",
        out_shape=jax.ShapeDtypeStruct((seqs, width), BF16),
        in_specs=[vmem] * len(small) + [anywhere] * 6,
        out_specs=vmem,
        scratch_shapes=[pltpu.VMEM((seqs, readout.shape[1]), F32)]
        + [pltpu.VMEM(array.shape, array.dtype) for array in weights]
        + [
            pltpu.VMEM((seqs, model), BF16),
            pltpu.VMEM((lanes - 1, seqs, width), BF16),
            pltpu.VMEM((groups // 4 * TILE, LANE), BF16),
            pltpu.VMEM((lanes, plane * TILE, LANE), BF16),
            pltpu.VMEM((CORES, model, 2 * hidden), BF16),
            pltpu.VMEM((CORES * hidden, model), BF16),
            pltpu.VMEM((lanes, plane * TILE, LANE), BF16),
            pltpu.VMEM((lanes - 1, plane * TILE, LANE), BF16),
            pltpu.VMEM((plane * TILE, LANE), BF16),
            pltpu.VMEM((plane * TILE, LANE), BF16),
            pltpu.SemaphoreType.REGULAR,
            dma((3,)),
            dma((3,)),
            dma((3,)),
            dma((3,)),
            dma((lanes - 1,)),
            dma((lanes - 1,)),
            dma,
            dma((GROUPS,)),
            dma((GROUPS, lanes - 1)),
            dma((GROUPS, lanes - 1)),
            dma((sum(map(len, PIECES)), lanes - 1)),
            dma((sum(map(len, PIECES)), lanes - 1)),
            dma,
            dma((2,)),
        ],
        compiler_params=pltpu.CompilerParams(collective_id=0, has_side_effects=True, vmem_limit_bytes=EXCHANGE_GRANT),
    )(*small, readout, *weights, expert_gate, expert_up, expert_down)


def local(
    tokens,
    recur_state,
    attn_gain,
    query_weight,
    key_weight,
    value_weight,
    outgate_weight,
    beta_weight,
    decay_weight,
    decay_rate,
    head_gain,
    output_weight,
    ffn_gain,
    routes,
    route_weight,
    expert_gate,
    expert_up,
    expert_down,
):
    readout, new_state = mixer(
        tokens, recur_state, attn_gain, query_weight, key_weight, value_weight, beta_weight, decay_weight, decay_rate
    )
    mixed = exchange(
        readout, tokens, attn_gain, head_gain, ffn_gain, routes, route_weight, outgate_weight, output_weight, expert_gate,
        expert_up, expert_down,
    )
    return (mixed, new_state)


def solution(mesh):
    return jax.shard_map(
        local,
        mesh=mesh,
        in_specs=(
            P("ep", None),
            P("ep", "tp", None, None),
            P(),
            P(None, "tp"),
            P(None, "tp"),
            P(None, "tp"),
            P(None, "tp"),
            P(),
            P(),
            P(),
            P(),
            P("tp", None),
            P(),
            P("ep", None),
            P("ep", None),
            P("ep", None, "tp"),
            P("ep", None, "tp"),
            P("ep", "tp", None),
        ),
        out_specs=(P("ep", "tp"), P("ep", "tp", None, None)),
        check_vma=False,
    )
```
